32 devices in a mesh: sp: 8 (over z, y), tp: 4 (over x, core).
Axes of the slice: x: 2, y: 2, z: 4, core: 2. Of those that a mesh axis runs over, the one named last changes fastest.
Arguments:
- residual_in: bfloat16 [6144, 2048], P('sp', 'tp'), may hold values from -11 to 11
- queries: bfloat16 [6144, 1024], P('sp', 'tp'), may hold values from -6 to 6
- keys: bfloat16 [6144, 256], P('sp'), may hold values from -6 to 6
- values: bfloat16 [6144, 256], P('sp'), may hold values from -6 to 6
- query_gain: float32 [128], replicated, may hold values from 1.5 to 5
- key_norm_gain: float32 [128], replicated, may hold values from 1.5 to 5
- out_weight: bfloat16 [1024, 2048], P('tp'), may hold values from -0.1875 to 0.1875
- mlp_gain: float32 [2048], replicated, may hold values from 0.1 to 1.9
- gate_weight: bfloat16 [2048, 5632], P('sp', 'tp'), may hold values from -0.125 to 0.125
- up_weight: bfloat16 [2048, 5632], P('sp', 'tp'), may hold values from -0.125 to 0.125
- down_weight: bfloat16 [5632, 2048], P('tp', 'sp'), may hold values from -0.15625 to 0.15625
Outputs:
- layer_out: bfloat16 [6144, 2048], P('sp', 'tp')
The draws below stay inside these ranges and needn't reach their ends.
All inputs are finite; a program needn't handle non-finite values.
Results may differ from the reference program's by a relative error of at most 0.012.
The reference program's roundings to bfloat16 on the way count: a program that leaves them out, or rounds other values in their place, can miss the bound.
Values may be sent and summed in bfloat16 or wider, within the bound.
A program may use at most 64 MiB of HBM per device.

```python
import math
import jax
import jax.numpy as jnp
from jax import lax

D = 2048
HEAD_SIZE = 128
QUERY_HEADS = 8
KEY_VALUE_HEADS = 2
FF = 5632
GRID = 64
TOK_DEV = 768
SEQUENCE_TOKENS = 6144
N_TP = 4


def draw_residual_in(key, part):
    column_scale = 0.5 * 4.0 ** (jnp.arange(D, dtype=jnp.float32) / D)
    rotary_period = jnp.clip(jax.random.normal(jax.random.fold_in(key, 3), (SEQUENCE_TOKENS, D)), -4.0, 4.0)
    return (rotary_period * column_scale).astype(jnp.bfloat16)


def draw_queries(key, part):
    rotary_period = jnp.clip(jax.random.normal(jax.random.fold_in(key, 1), (SEQUENCE_TOKENS, QUERY_HEADS * HEAD_SIZE)), -4.0, 4.0)
    return jnp.clip(rotary_period, -6.0, 6.0).astype(jnp.bfloat16)


def draw_keys(key, part):
    rotary_period = jnp.clip(jax.random.normal(jax.random.fold_in(key, 2), (SEQUENCE_TOKENS, KEY_VALUE_HEADS * HEAD_SIZE)), -4.0, 4.0)
    return jnp.clip(rotary_period, -6.0, 6.0).astype(jnp.bfloat16)


def draw_gain(key, salt):
    return jnp.exp(jax.random.uniform(jax.random.fold_in(key, salt), (HEAD_SIZE,), jnp.float32, math.log(1.5), math.log(3.0)))


def draw_query_gain(key, part):
    return draw_gain(key, 4)


def draw_key_norm_gain(key, part):
    return draw_gain(key, 5)


def steps_of(stream_key, extent, cuts, low, top_value):
    loudness, own = 1.0, jax.random.fold_in(stream_key, 6)
    for dim, shards_of in cuts:
        steps = jnp.exp(jax.random.uniform(jax.random.fold_in(own, dim), (shards_of,), jnp.float32, low / len(cuts), top_value / len(cuts)))
        loudness = loudness * jnp.repeat(steps, extent[dim] // shards_of).reshape([-1 if axis == dim else 1 for axis in range(len(extent))])
    return loudness


def gaussian(key, extent, spread, limit, cuts=(), kind=jnp.bfloat16):
    drawn = jax.random.normal(key, extent, jnp.float32) * spread
    if len(cuts) > 0:
        drawn = steps_of(key, extent, cuts, -0.22, 0.18) * drawn
    return jnp.clip(drawn, min=-limit, max=limit).astype(kind)


def setup_inputs(seed: int = 0) -> dict:
    key_of = jax.random.split(jax.random.key(seed), 12)
    return {
        "residual_in": draw_residual_in(jax.random.fold_in(key_of[11], 71), 0),
        "queries": draw_queries(jax.random.fold_in(key_of[11], 71), 0),
        "keys": draw_keys(jax.random.fold_in(key_of[11], 71), 0),
        "values": gaussian(key_of[3], (SEQUENCE_TOKENS, KEY_VALUE_HEADS * HEAD_SIZE), 1.0, 6.0, ((0, 8),)),
        "query_gain": draw_query_gain(jax.random.fold_in(key_of[11], 71), 0),
        "key_norm_gain": draw_key_norm_gain(jax.random.fold_in(key_of[11], 71), 0),
        "out_weight": gaussian(key_of[6], (QUERY_HEADS * HEAD_SIZE, D), (QUERY_HEADS * HEAD_SIZE) ** -0.5, 0.1875, ((0, 4),)),
        "mlp_gain": jnp.clip(1.0 + 0.18 * jax.random.normal(key_of[7], (D,), jnp.float32), 0.1, 1.9),
        "gate_weight": gaussian(key_of[8], (D, FF), D ** -0.5, 0.125, ((0, 8), (1, 4))),
        "up_weight": gaussian(key_of[9], (D, FF), D ** -0.5, 0.125, ((0, 8), (1, 4))),
        "down_weight": gaussian(key_of[10], (FF, D), (FF // 4) ** -0.5, 0.15625, ((0, 4), (1, 8))),
    }


eps = 1e-06
rotary_base = 10000.0

def apply_rotary(vectors, grid_positions):
    half_size = vectors.shape[-1] // 2
    frequency = rotary_base ** (-jnp.arange(0, half_size, 2, dtype=jnp.float32) / half_size)
    grid_row = (grid_positions // GRID).astype(jnp.float32)
    grid_col = (grid_positions % GRID).astype(jnp.float32)
    angles = jnp.concatenate([grid_row[:, None] * frequency, grid_col[:, None] * frequency], axis=-1)[:, None, :]
    cosine_table = jnp.cos(angles)
    sine_table = jnp.sin(angles)
    first_half = vectors[..., :half_size]
    second_half = vectors[..., half_size:]
    return jnp.concatenate([first_half * cosine_table - second_half * sine_table, first_half * sine_table + second_half * cosine_table], axis=-1)

def per_head_norm(vectors, gain):
    return vectors * lax.rsqrt(lax.optimization_barrier(jnp.mean(vectors * vectors, axis=-1, keepdims=True)) + eps) * gain

def grouped_sum(left, right, groups):
    group_width = left.shape[1] // groups

    def add_group(running, group_index):
        left_part = lax.dynamic_slice_in_dim(left, group_index * group_width, group_width, 1)
        right_part = lax.dynamic_slice_in_dim(right, group_index * group_width, group_width, 0)
        partial_sum = jnp.dot(left_part, right_part, preferred_element_type=jnp.float32)
        rounded = lax.optimization_barrier(partial_sum.astype(jnp.bfloat16))
        return (running + rounded.astype(jnp.float32), None)
    start_value = jnp.zeros((left.shape[0], right.shape[1]), jnp.float32)
    result, ignored = lax.scan(add_group, start_value, jnp.arange(groups, dtype=jnp.int32))
    return result

def reference(residual_in, queries, keys, values, query_gain, key_norm_gain, out_weight, mlp_gain, gate_weight, up_weight, down_weight):
    grid_positions = jnp.arange(SEQUENCE_TOKENS, dtype=jnp.int32)
    queries_per_group = QUERY_HEADS // KEY_VALUE_HEADS
    query_rows = apply_rotary(per_head_norm(queries.astype(jnp.float32).reshape(SEQUENCE_TOKENS, QUERY_HEADS, HEAD_SIZE), query_gain), grid_positions).astype(jnp.bfloat16)
    key_matrix = apply_rotary(per_head_norm(keys.astype(jnp.float32).reshape(SEQUENCE_TOKENS, KEY_VALUE_HEADS, HEAD_SIZE), key_norm_gain), grid_positions).astype(jnp.bfloat16)
    value_matrix = values.reshape(SEQUENCE_TOKENS, KEY_VALUE_HEADS, HEAD_SIZE)
    score_scale = HEAD_SIZE ** (-0.5)

    def one_head(head_index):
        head_queries = lax.dynamic_index_in_dim(query_rows, head_index, 1, keepdims=False)
        shared = head_index // queries_per_group
        head_keys = lax.dynamic_index_in_dim(key_matrix, shared, 1, keepdims=False)
        head_values = lax.dynamic_index_in_dim(value_matrix, shared, 1, keepdims=False)

        def one_block(first_row):
            block_queries = lax.dynamic_slice_in_dim(head_queries, first_row, TOK_DEV, 0)
            scores = jnp.dot(block_queries, head_keys.T, preferred_element_type=jnp.float32) * score_scale
            row_max = lax.optimization_barrier(jnp.max(scores, axis=1, keepdims=True))
            weights = jnp.exp(scores - row_max)
            row_sum = lax.optimization_barrier(jnp.sum(weights, axis=1, keepdims=True))
            weighted = jnp.dot(weights.astype(jnp.bfloat16), head_values, preferred_element_type=jnp.float32)
            return (weighted / row_sum).astype(jnp.bfloat16)
        starts = jnp.arange(0, SEQUENCE_TOKENS, TOK_DEV, dtype=jnp.int32)
        return lax.map(one_block, starts).reshape(SEQUENCE_TOKENS, HEAD_SIZE)
    heads_out = lax.map(one_head, jnp.arange(QUERY_HEADS, dtype=jnp.int32))
    attended = jnp.transpose(heads_out, (1, 0, 2)).reshape(SEQUENCE_TOKENS, QUERY_HEADS * HEAD_SIZE)
    projected = grouped_sum(attended, out_weight, N_TP)
    residual_mid = residual_in.astype(jnp.float32) + projected
    normed = (residual_mid * lax.rsqrt(lax.optimization_barrier(jnp.mean(residual_mid * residual_mid, axis=1, keepdims=True)) + eps) * mlp_gain).astype(jnp.bfloat16)
    gate_out = jnp.dot(normed, gate_weight, preferred_element_type=jnp.float32)
    up_out = jnp.dot(normed, up_weight, preferred_element_type=jnp.float32)
    hidden = (jax.nn.silu(gate_out) * up_out).astype(jnp.bfloat16)
    down_sum = grouped_sum(hidden, down_weight, N_TP)
    return (residual_mid + 0.5 * down_sum).astype(jnp.bfloat16)
```

```python
import functools
import jax
import jax.numpy as jnp
from jax import lax
from jax.experimental import pallas as pl
from jax.experimental.pallas import tpu as pltpu
from jax.sharding import PartitionSpec as P

D = 2048
HEAD_SIZE = 128
QUERY_HEADS = 8
KEY_VALUE_HEADS = 2
GRID = 64

eps = 1e-06
rotary_base = 10000.0
MESH = pl.DeviceIdType.MESH
VMEM_LIMIT = 60 * 1024 * 1024
F32 = jnp.float32
BF16 = jnp.bfloat16


def apply_rotary(vectors, grid_positions):
    half_size = vectors.shape[-1] // 2
    frequency = rotary_base ** (-jnp.arange(0, half_size, 2, dtype=F32) / half_size)
    grid_row = (grid_positions // GRID).astype(F32)
    grid_col = (grid_positions % GRID).astype(F32)
    angles = jnp.concatenate(
        [grid_row[:, None] * frequency, grid_col[:, None] * frequency], axis=-1
    )[:, None, :]
    cosine_table = jnp.cos(angles)
    sine_table = jnp.sin(angles)
    first_half = vectors[..., :half_size]
    second_half = vectors[..., half_size:]
    return jnp.concatenate(
        [
            first_half * cosine_table - second_half * sine_table,
            first_half * sine_table + second_half * cosine_table,
        ],
        axis=-1,
    )


def per_head_norm(vectors, gain):
    return vectors * lax.rsqrt(jnp.mean(vectors * vectors, axis=-1, keepdims=True) + eps) * gain


def remote(src, dst, send, recv, sp, tp):
    copy = pltpu.make_async_remote_copy(
        src_ref=src, dst_ref=dst, send_sem=send, recv_sem=recv,
        device_id={"sp": sp, "tp": tp}, device_id_type=MESH,
    )
    copy.start()
    return copy


def greet(peers):
    barrier = pltpu.get_barrier_semaphore()
    for sp, tp in peers:
        pl.semaphore_signal(
            barrier, inc=1, device_id={"sp": sp, "tp": tp}, device_id_type=MESH
        )
    pl.semaphore_wait(barrier, len(peers))


def place():
    sp = lax.axis_index("sp")
    tp = lax.axis_index("tp")
    return sp, tp, sp // 2, lax.rem(sp, 2), tp // 2, lax.rem(tp, 2)


def rows_at(index, size):
    return pl.ds(pl.multiple_of(index * size, size), size)


def layer_kernel(nz, nx, heads, q_ref, kv_ref, w_ref, res_ref, gain_ref, gu_ref, dn_ref,
                 mid_ref, normed_ref, gu_out, dn_out,
                 kvs, vt, top_s, sum_s, acc_s, proj, from_core, outgo, from_x, squares, block,
                 s_z, r_z, s_y, r_y, s_c, r_c, s1, r1, s2, r2, s3, r3,
                 s_ax, r_ax, s_az, r_az, s_ar, r_ar, s_ac, r_ac,
                 s_gz, r_gz, s_gy, r_gy, s_dz, r_dz, s_dy, r_dy):
    sp, tp, z, y, x, c = place()
    rows, own = res_ref.shape
    n_tp = 2 * nx
    half = rows // 2
    tile = 256 if rows % 256 == 0 else rows
    tiles = rows // tile
    other = x * 2 + 1 - c
    u = lax.rem(z, 2)
    z_at = [lax.rem(z + k, nz) for k in range(nz)]
    z_from = [lax.rem(z - k + nz, nz) for k in range(nz)]
    xs = [lax.rem(x + j, nx) for j in range(nx)]
    back = [lax.rem(x - j + nx, nx) for j in range(nx)]
    y_peer = (z * 2 + 1 - y, tp)
    core_peer = (sp, other)
    z_pair = ((z + 1 - 2 * u) * 2 + y, tp)
    z_peers = [(z_at[k] * 2 + y, tp) for k in range(1, nz)]
    row_peers = [(sp, xs[j] * 2 + c) for j in range(1, nx)]
    across = [(sp, xs[j] * 2 + 1 - c) for j in range(1, nx)]
    greet(z_peers + [y_peer, core_peer] + row_peers + across)

    def spot(owner, side):
        return kvs.at[pl.ds(pl.multiple_of(owner * rows + side * half, half), half), :]

    sends = []

    def send(src, dst, out, arrive, slot, to):
        copy = remote(src, dst, out.at[slot], arrive.at[slot], *to)
        sends.append(copy)
        return copy

    mine = kv_ref.at[rows_at(c, half), :]
    kz = [None] + [send(mine, spot(sp, c), s_z, r_z, k - 1, z_peers[k - 1]) for k in range(1, nz)]
    ky = [send(mine, spot(sp, c), s_y, r_y, 0, y_peer)]
    gz = [None] + [
        send(gu_ref.at[lax.rem(z_at[k], 2)], gu_out.at[rows_at(sp, gu_ref.shape[1]), :],
             s_gz, r_gz, k - 1, z_peers[k - 1])
        for k in range(1, nz)
    ]
    kvs[rows_at(sp, rows), :] = kv_ref[...]
    depth = gu_ref.shape[1]
    wide = dn_ref.shape[2]
    gu_out[rows_at(sp, depth), :] = gu_ref[u]
    dn_out[:, rows_at(sp, wide)] = dn_ref[u]

    top_s[...] = jnp.full(top_s.shape, -1e30, F32)
    sum_s[...] = jnp.zeros(sum_s.shape, F32)
    acc_s[...] = jnp.zeros(acc_s.shape, F32)
    factor = HEAD_SIZE ** (-0.5) * 1.4426950408889634

    def attend(owner):
        at = rows_at(owner, rows)
        vt[...] = kvs[at, HEAD_SIZE:].astype(F32).T.astype(BF16)

        @pl.loop(0, tiles)
        def _(i):
            for h in range(heads):
                q = q_ref[rows_at(i, tile), h * HEAD_SIZE : (h + 1) * HEAD_SIZE]
                s = lax.dot_general(
                    kvs[at, 0:HEAD_SIZE], q, (((1,), (1,)), ((), ())), preferred_element_type=F32
                )
                n = i * heads + h
                top = top_s[n]
                new_top = jnp.maximum(top, jnp.max(s, axis=0, keepdims=True))
                fade = jnp.exp2((top - new_top) * factor)
                w = jnp.exp2((s - new_top) * factor)
                top_s[n] = new_top
                sum_s[n] = sum_s[n] * fade + jnp.sum(w, axis=0, keepdims=True)
                acc_s[n] = acc_s[n] * fade + jnp.dot(
                    vt[...], w.astype(BF16), preferred_element_type=F32
                )

    kc = {}

    def over(k, side):
        owner = z_from[k] * 2 + side
        slot = 2 * k + (0 if side is y else 1)
        return owner, slot

    def to_core(k, row, slot):
        block_at = spot(z_from[k] * 2 + row, c)
        kc[slot] = send(block_at, block_at, s_c, r_c, slot, core_peer)

    def near_arrived(k):
        kz[k].wait_recv()
        block_at = spot(z_from[k] * 2 + y, c)
        ky.append(send(block_at, block_at, s_y, r_y, k, y_peer))
        to_core(k, y, 2 * k - 1)

    def far_arrived(k):
        ky[k].wait_recv()
        to_core(k, 1 - y, 2 * k)

    def use(slot, owner):
        kc[slot].wait_recv()
        attend(owner)

    attend(sp)
    far_arrived(0)
    if nz > 1:
        near_arrived(1)
    use(0, z * 2 + 1 - y)
    for k in range(1, nz):
        if k + 1 < nz:
            near_arrived(k + 1)
        else:
            far_arrived(1)
        use(2 * k - 1, z_from[k] * 2 + y)
    gy = [send(gu_ref.at[u], gu_out.at[rows_at(sp, depth), :], s_gy, r_gy, 0, y_peer)]
    for k in range(1, nz):
        if k + 1 < nz:
            far_arrived(k + 1)
        use(2 * k, z_from[k] * 2 + 1 - y)

    def cols(t):
        return rows_at(t, own)

    @pl.loop(0, tiles)
    def _(i):
        parts = [
            (acc_s[i * heads + h] / sum_s[i * heads + h]).astype(BF16) for h in range(heads)
        ]
        got = jnp.concatenate(parts, axis=0) if heads > 1 else parts[0]
        proj[rows_at(i, tile), :] = lax.dot_general(
            got, w_ref[...], (((0,), (0,)), ((), ())), preferred_element_type=F32
        ).astype(BF16)

    step = rows // 8
    near = [
        send(proj.at[:, cols(xs[j] * 2 + 1 - c)], from_core.at[j], s1, r1, j, core_peer)
        for j in list(range(1, nx)) + [0]
    ]
    near = [near[-1]] + near[:-1]
    to_x = []
    for j in range(1, nx):
        near[j].wait_recv()

        @pl.loop(0, 8)
        def _(i):
            at = rows_at(i, step)
            outgo[j - 1, at, :] = (
                proj[at, cols(xs[j] * 2 + c)].astype(F32) + from_core[j, at, :].astype(F32)
            ).astype(BF16)

        to_x.append(send(outgo.at[j - 1], from_x.at[j - 1], s2, r2, j - 1, row_peers[j - 1]))
    near[0].wait_recv()

    def relay_gu(k):
        gz[k].wait_recv()
        at = gu_out.at[rows_at(z_from[k] * 2 + y, depth), :]
        gy.append(send(at, at, s_gy, r_gy, k, y_peer))

    for copy in to_x:
        copy.wait_recv()
    ones = jnp.ones((8, own), F32)

    for i in range(tiles):
        at = pl.ds(i * tile, tile)
        total = proj[at, cols(tp)].astype(F32) + from_core[0, at, :].astype(F32)
        for j in range(1, nx):
            total += from_x[j - 1, at, :].astype(F32)
        mid = res_ref[at, :].astype(F32) + total
        mid_ref[at, :] = mid
        squares[0, :, at] = lax.dot_general(
            ones, mid * mid, (((1,), (1,)), ((), ())),
            precision=lax.Precision.HIGHEST, preferred_element_type=F32,
        )
    peers = [core_peer] + row_peers + across
    sq = [send(squares.at[0], squares.at[k + 1], s3, r3, k, peers[k]) for k in range(len(peers))]
    for copy in sq:
        copy.wait_recv()

    def home(uu, t):
        return normed_ref.at[rows_at(uu, rows), cols(t)]

    for i in range(tiles):
        at = pl.ds(i * tile, tile)
        square = squares[0, :, at]
        for k in range(len(peers)):
            square += squares[k + 1, :, at]
        scale = lax.rsqrt(square.T[:, 0:1] / (n_tp * own) + eps)
        block[at, :] = (mid_ref[at, :] * scale * gain_ref[...]).astype(BF16)
    az = send(block, home(u, tp), s_az, r_az, 0, z_pair)
    ax = [send(block, home(u, tp), s_ax, r_ax, j - 1, row_peers[j - 1]) for j in range(1, nx)]
    ac = [send(block, home(u, tp), s_ac, r_ac, 0, core_peer)]
    normed_ref[rows_at(u, rows), cols(tp)] = block[...]
    dz = [None] + [
        send(dn_ref.at[lax.rem(z_at[k], 2)], dn_out.at[:, rows_at(sp, wide)],
             s_dz, r_dz, k - 1, z_peers[k - 1])
        for k in range(1, nz)
    ]

    def on_core(uu, t, slot):
        at = home(uu, t)
        ac.append(send(at, at, s_ac, r_ac, slot, core_peer))

    relay_gu(1)
    for j in range(1, nx):
        ax[j - 1].wait_recv()
        on_core(u, back[j] * 2 + c, j)
    az.wait_recv()
    there = home(1 - u, tp)
    ar = [send(there, there, s_ar, r_ar, j - 1, row_peers[j - 1]) for j in range(1, nx)]
    on_core(1 - u, tp, nx)
    for k in range(2, nz):
        relay_gu(k)
    dy = [send(dn_ref.at[u], dn_out.at[:, rows_at(sp, wide)], s_dy, r_dy, 0, y_peer)]
    for j in range(1, nx):
        ar[j - 1].wait_recv()
        on_core(1 - u, back[j] * 2 + c, nx + j)
    for k in range(1, nz):
        dz[k].wait_recv()
        at = dn_out.at[:, rows_at(z_from[k] * 2 + y, wide)]
        dy.append(send(at, at, s_dy, r_dy, k, y_peer))
    for copy in ac + gy + dy:
        copy.wait_recv()
    for copy in sends:
        copy.wait_send()


def layer(q, kv, w, res, gain, gu, dn, n_sp, n_tp):
    nz, nx = n_sp // 2, n_tp // 2
    rows, own = res.shape
    heads = q.shape[1] // HEAD_SIZE
    tile = 256 if rows % 256 == 0 else rows
    count = heads * (rows // tile)
    width = n_tp * own
    dma = pltpu.SemaphoreType.DMA
    n = 2 * nx
    vm = pl.BlockSpec(memory_space=pltpu.VMEM)

    def two(k):
        return [dma((k,)), dma((k,))]

    return pl.pallas_call(
        functools.partial(layer_kernel, nz, nx, heads),
        out_shape=(
            jax.ShapeDtypeStruct((rows, own), F32),
            jax.ShapeDtypeStruct((2 * rows, width), BF16),
            jax.ShapeDtypeStruct((n_sp * gu.shape[1], gu.shape[2]), BF16),
            jax.ShapeDtypeStruct((dn.shape[1], n_sp * dn.shape[2]), BF16),
        ),
        in_specs=[vm] * 7,
        out_specs=(vm,) * 4,
        scratch_shapes=[
            pltpu.VMEM((n_sp * rows, 2 * HEAD_SIZE), BF16),
            pltpu.VMEM((HEAD_SIZE, rows), BF16),
            pltpu.VMEM((count, 1, tile), F32),
            pltpu.VMEM((count, 1, tile), F32),
            pltpu.VMEM((count, HEAD_SIZE, tile), F32),
            pltpu.VMEM((rows, width), BF16),
            pltpu.VMEM((nx, rows, own), BF16),
            pltpu.VMEM((nx - 1, rows, own), BF16),
            pltpu.VMEM((nx - 1, rows, own), BF16),
            pltpu.VMEM((n, 8, rows), F32),
            pltpu.VMEM((rows, own), BF16),
        ] + two(nz - 1) + two(nz) + two(2 * nz - 1) + two(nx) + two(nx - 1) + two(n - 1)
        + two(nx - 1) + two(1) + two(nx - 1) + two(2 * nx)
        + two(nz - 1) + two(nz) + two(nz - 1) + two(nz),
        compiler_params=pltpu.CompilerParams(
            collective_id=0, has_side_effects=True, vmem_limit_bytes=VMEM_LIMIT
        ),
        name="layer",
    )(q, kv, w, res, gain, gu, dn)


def down_kernel(nx, terms_ref, mid_ref, out_ref, from_core, outgo, from_y, from_x, relay,
                last_x, last_y, s1, r1, s2, r2, s3, r3, s4, r4, s5, r5):
    sp, tp, z, row, x, c = place()
    rows, own = mid_ref.shape
    half = rows // 2
    top, low = pl.ds(0, half), pl.ds(half, half)
    other = x * 2 + 1 - c
    y = lax.rem(z, 2)
    y_peer = ((z + 1 - 2 * y) * 2 + row, tp)
    xs = [lax.rem(x + j, nx) for j in range(nx)]
    x_peers = [(sp, xs[j] * 2 + c) for j in range(nx)]
    greet([(sp, other), y_peer] + x_peers[1:])
    every = [(1 - y, xs[j]) for j in range(nx)] + [(y, xs[j]) for j in range(1, nx)] + [(y, x)]
    order = list(range(1, 2 * nx - 1)) + [0, 2 * nx - 1]

    def cols(t):
        return pl.ds(pl.multiple_of(t * own, own), own)

    near = {}
    for k in order:
        yy, xx = every[k]
        near[k] = remote(
            terms_ref.at[pl.ds(pl.multiple_of(yy * rows, rows), rows), cols(xx * 2 + 1 - c)],
            from_core.at[k], s1.at[k], r1.at[k], sp, other)
    step = rows // 8
    to_y, to_x, again = {}, {}, []
    for k in order[:-1]:
        yy, xx = every[k]
        near[k].wait_recv()

        @pl.loop(0, 8)
        def _(i):
            at = pl.ds(pl.multiple_of(i * step, step), step)
            here = pl.ds(pl.multiple_of(yy * rows + i * step, step), step)
            outgo[k, at, :] = (
                terms_ref[here, cols(xx * 2 + c)].astype(F32) + from_core[k, at, :].astype(F32)
            ).astype(BF16)

        if k < nx:
            to_y[k] = remote(outgo.at[k, top], from_y.at[k], s2.at[k], r2.at[k], *y_peer)
        j = k if k < nx else k - nx + 1
        if j > 0:
            slot = 2 * (j - 1) + (1 if k < nx else 0)
            to_x[slot] = remote(outgo.at[k, low], from_x.at[slot], s3.at[slot], r3.at[slot],
                                *x_peers[j])
    for j in range(1, nx):
        to_y[j].wait_recv()

        @pl.loop(0, 4)
        def _(i):
            at = pl.ds(pl.multiple_of(i * step, step), step)
            relay[j, at, :] = (
                outgo[nx + j - 1, at, :].astype(F32) + from_y[j, at, :].astype(F32)
            ).astype(BF16)

        again.append(remote(relay.at[j], last_x.at[j - 1], s4.at[j - 1], r4.at[j - 1],
                            *x_peers[j]))
    for j in range(1, nx):
        to_x[2 * j - 1].wait_recv()

    @pl.loop(0, 4)
    def _(i):
        at = pl.ds(pl.multiple_of(i * step, step), step)
        here = pl.ds(pl.multiple_of(half + i * step, step), step)
        total = outgo[0, here, :].astype(F32)
        for j in range(1, nx):
            total += from_x[2 * j - 1, at, :].astype(F32)
        relay[0, at, :] = total.astype(BF16)

    again.append(remote(relay.at[0], last_y, s5.at[0], r5.at[0], *y_peer))
    near[2 * nx - 1].wait_recv()
    to_y[0].wait_recv()
    for j in range(1, nx):
        to_x[2 * j - 2].wait_recv()
    for copy in again:
        copy.wait_recv()

    @pl.loop(0, 4)
    def _(i):
        at = pl.ds(pl.multiple_of(i * step, step), step)
        for part in range(2):
            to = pl.ds(pl.multiple_of(part * half + i * step, step), step)
            here = pl.ds(pl.multiple_of(y * rows + part * half + i * step, step), step)
            total = terms_ref[here, cols(tp)].astype(F32)
            total += from_core[2 * nx - 1, to, :].astype(F32)
            total += (from_y[0, at, :] if part == 0 else last_y[at, :]).astype(F32)
            for j in range(1, nx):
                total += (last_x[j - 1, at, :] if part == 0
                          else from_x[2 * j - 2, at, :]).astype(F32)
            out_ref[to, :] = (mid_ref[to, :] + 0.5 * total).astype(BF16)

    for copy in list(near.values()) + list(to_y.values()) + list(to_x.values()) + again:
        copy.wait_send()


def down_sum(terms, mid, n_tp):
    nx = n_tp // 2
    rows, own = mid.shape
    dma = pltpu.SemaphoreType.DMA
    n = 2 * nx
    vm = pl.BlockSpec(memory_space=pltpu.VMEM)
    return pl.pallas_call(
        functools.partial(down_kernel, nx),
        out_shape=jax.ShapeDtypeStruct((rows, own), BF16),
        in_specs=[vm] * 2,
        out_specs=vm,
        scratch_shapes=[
            pltpu.VMEM((n, rows, own), BF16),
            pltpu.VMEM((n - 1, rows, own), BF16),
            pltpu.VMEM((nx, rows // 2, own), BF16),
            pltpu.VMEM((n - 2, rows // 2, own), BF16),
            pltpu.VMEM((nx, rows // 2, own), BF16),
            pltpu.VMEM((nx - 1, rows // 2, own), BF16),
            pltpu.VMEM((rows // 2, own), BF16),
            dma((n,)), dma((n,)), dma((nx,)), dma((nx,)), dma((n - 2,)), dma((n - 2,)),
            dma((nx - 1,)), dma((nx - 1,)), dma((1,)), dma((1,)),
        ],
        compiler_params=pltpu.CompilerParams(
            collective_id=1, has_side_effects=True, vmem_limit_bytes=VMEM_LIMIT
        ),
        name="down_sum",
    )(terms, mid)


def on_device(n_sp, n_tp, residual_in, queries, keys, values, query_gain, key_norm_gain,
              out_weight, mlp_gain, gate_weight, up_weight, down_weight):
    local_rows = residual_in.shape[0]
    local_heads = queries.shape[1] // HEAD_SIZE
    queries_per_group = QUERY_HEADS // KEY_VALUE_HEADS
    tp_index = lax.axis_index("tp")
    sp_index = lax.axis_index("sp")
    units = gate_weight.shape[1] // 2
    gate_up = jnp.stack([
        jnp.concatenate(
            [w[:, part * units : (part + 1) * units] for w in (gate_weight, up_weight)], axis=1
        )
        for part in range(2)
    ])
    down = down_weight.reshape(2, units, down_weight.shape[1])

    grid_positions = sp_index * local_rows + jnp.arange(local_rows, dtype=jnp.int32)
    shared = tp_index * local_heads // queries_per_group
    own_keys = lax.dynamic_slice_in_dim(keys, shared * HEAD_SIZE, HEAD_SIZE, 1)
    own_values = lax.dynamic_slice_in_dim(values, shared * HEAD_SIZE, HEAD_SIZE, 1)
    key_matrix = apply_rotary(
        per_head_norm(own_keys.astype(F32)[:, None, :], key_norm_gain), grid_positions
    )[:, 0, :].astype(BF16)
    query_rows = apply_rotary(
        per_head_norm(queries.astype(F32).reshape(local_rows, local_heads, HEAD_SIZE), query_gain),
        grid_positions,
    ).astype(BF16).reshape(local_rows, local_heads * HEAD_SIZE)
    own_kv = jnp.concatenate([key_matrix, own_values], axis=1)
    own_width = residual_in.shape[1]
    gain_own = lax.dynamic_slice_in_dim(mlp_gain, tp_index * own_width, own_width, 0)[None, :]
    residual_mid, normed, gate_up, down = layer(
        query_rows, own_kv, out_weight, residual_in, gain_own, gate_up, down, n_sp, n_tp
    )
    gate_up = jnp.dot(normed, gate_up, preferred_element_type=F32)
    hidden = (jax.nn.silu(gate_up[:, :units]) * gate_up[:, units:]).astype(BF16)
    down_terms = jnp.dot(hidden, down, preferred_element_type=F32).astype(BF16)
    return down_sum(down_terms, residual_mid, n_tp)


def solution(mesh):
    in_specs = (
        P("sp", "tp"),
        P("sp", "tp"),
        P("sp", None),
        P("sp", None),
        P(),
        P(),
        P("tp", None),
        P(),
        P("sp", "tp"),
        P("sp", "tp"),
        P("tp", "sp"),
    )
    out_specs = P("sp", "tp")
    return jax.shard_map(
        functools.partial(on_device, mesh.shape["sp"], mesh.shape["tp"]),
        mesh=mesh, in_specs=in_specs, out_specs=out_specs, check_vma=False,
    )
```

```python
import functools
import jax
import numpy as np
import jax.numpy as jnp
from jax import lax
from jax.experimental import pallas as pl
from jax.experimental.pallas import tpu as pltpu
from jax.sharding import PartitionSpec as P

D = 2048
HEAD_SIZE = 128
QUERY_HEADS = 8
KEY_VALUE_HEADS = 2
GRID = 64

eps = 1e-06
rotary_base = 10000.0
MESH = pl.DeviceIdType.MESH
VMEM_LIMIT = 67043328
F32 = jnp.float32
BF16 = jnp.bfloat16


def remote(src, dst, send, recv, sp, tp):
    copy = pltpu.make_async_remote_copy(
        src_ref=src, dst_ref=dst, send_sem=send, recv_sem=recv,
        device_id={"sp": sp, "tp": tp}, device_id_type=MESH,
    )
    copy.start()
    return copy


def greet(peers):
    barrier = pltpu.get_barrier_semaphore()
    for sp, tp in peers:
        pl.semaphore_signal(
            barrier, inc=1, device_id={"sp": sp, "tp": tp}, device_id_type=MESH
        )
    pl.semaphore_wait(barrier, len(peers))


def place():
    sp = lax.axis_index("sp")
    tp = lax.axis_index("tp")
    return sp, tp, sp // 2, lax.rem(sp, 2), tp // 2, lax.rem(tp, 2)


def rows_at(index, size):
    return pl.ds(pl.multiple_of(index * size, size), size)


def rotary_tables(tokens):
    half_size = HEAD_SIZE // 2
    frequency = np.float32(rotary_base) ** (
        -np.arange(0, half_size, 2, dtype=np.float32) / np.float32(half_size)
    )
    longest = max(tokens // GRID, GRID)
    angles = np.arange(longest, dtype=np.float32)[:, None] * frequency.astype(np.float32)
    cosine, sine = np.cos(angles), np.sin(angles)
    none = np.zeros_like(angles)
    rows = tokens // GRID
    pieces = [
        np.concatenate([cosine, none, cosine, none], axis=1)[:rows],
        np.concatenate([none, cosine, none, cosine], axis=1)[:GRID],
        np.concatenate([-sine, none, sine, none], axis=1)[:rows],
        np.concatenate([none, -sine, none, sine], axis=1)[:GRID],
    ]
    return [jnp.asarray(piece, F32) for piece in pieces]


def layer_kernel(nz, nx, heads, q_in, k_in, v_in, q_gain, k_gain, w_ref, res_ref, gain_ref,
                 gate_ref, up_ref, dn_ref, cos_row, cos_col, sin_row, sin_col,
                 out_ref,
                 q_ref, kv_ref, kvs, vt, top_s, sum_s, acc_s, proj, from_core, outgo, from_x,
                 squares, block, mid_ref, normed_ref, gu_ref, gu_all, dn_all, gu_acc, hidden,
                 terms, d_core, d_out, d_y, d_x, relay, last_x, last_y,
                 s_z, r_z, s_y, r_y, s_c, r_c, s1, r1, s2, r2, s3, r3,
                 s_ax, r_ax, s_az, r_az, s_ar, r_ar, s_ac, r_ac,
                 s_gz, r_gz, s_gy, r_gy, s_dz, r_dz, s_dy, r_dy,
                 e1, f1, e2, f2, e3, f3, e4, f4, e5, f5):
    sp, tp, z, y, x, c = place()
    rows, own = res_ref.shape
    n_tp = 2 * nx
    half = rows // 2
    tile = 256 if rows % 256 == 0 else rows
    tiles = rows // tile
    depth, twice = gate_ref.shape
    units = twice // 2
    wide = dn_ref.shape[2]
    other = x * 2 + 1 - c
    u = lax.rem(z, 2)
    z_at = [lax.rem(z + k, nz) for k in range(nz)]
    z_from = [lax.rem(z - k + nz, nz) for k in range(nz)]
    xs = [lax.rem(x + j, nx) for j in range(nx)]
    back = [lax.rem(x - j + nx, nx) for j in range(nx)]
    y_peer = (z * 2 + 1 - y, tp)
    core_peer = (sp, other)
    z_other = z + 1 - 2 * u
    z_pair = (z_other * 2 + y, tp)
    z_peers = [(z_at[k] * 2 + y, tp) for k in range(1, nz)]
    row_peers = [(sp, xs[j] * 2 + c) for j in range(1, nx)]
    across = [(sp, xs[j] * 2 + 1 - c) for j in range(1, nx)]

    def turn(ref, gain, columns, i):
        at = rows_at(i, GRID)
        v = ref[at, columns].astype(F32)
        v = v * lax.rsqrt(jnp.mean(v * v, axis=1, keepdims=True) + eps) * gain[...]
        row = sp * (rows // GRID) + i
        cosine = cos_row[pl.ds(row, 1), :] + cos_col[...]
        sine = sin_row[pl.ds(row, 1), :] + sin_col[...]
        return at, (v * cosine + pltpu.roll(v, HEAD_SIZE // 2, 1) * sine).astype(BF16)

    with jax.named_scope("prep"):
        shared = pl.ds(
            pl.multiple_of(tp * heads // (QUERY_HEADS // KEY_VALUE_HEADS) * HEAD_SIZE, HEAD_SIZE),
            HEAD_SIZE,
        )

        @pl.loop(0, rows // GRID)
        def _(i):
            at, turned = turn(k_in, k_gain, shared, i)
            kv_ref[at, 0:HEAD_SIZE] = turned
            kv_ref[at, HEAD_SIZE:] = v_in[at, shared]

        for part in range(2):
            cut = slice(part * units, (part + 1) * units)
            for i in range(0, depth, 64):
                gu_ref[part, i : i + 64, :] = jnp.concatenate(
                    [gate_ref[i : i + 64, cut].astype(F32), up_ref[i : i + 64, cut].astype(F32)],
                    axis=1,
                ).astype(BF16)

    with jax.named_scope("greet"):
        greet(z_peers + [y_peer, core_peer] + row_peers + across)

    def spot(owner, side):
        return kvs.at[pl.ds(pl.multiple_of(owner * rows + side * half, half), half), :]

    sends = []

    def send(src, dst, out, arrive, slot, to):
        copy = remote(src, dst, out.at[slot], arrive.at[slot], *to)
        sends.append(copy)
        return copy

    def got(name, copy):
        with jax.named_scope("w_" + name):
            copy.wait_recv()

    mine = kv_ref.at[rows_at(c, half), :]
    kz = [None] + [send(mine, spot(sp, c), s_z, r_z, k - 1, z_peers[k - 1]) for k in range(1, nz)]
    ky = [send(mine, spot(sp, c), s_y, r_y, 0, y_peer)]
    kvs[rows_at(sp, rows), :] = kv_ref[...]
    gu_all[rows_at(sp, depth), :] = gu_ref[u]
    dn_all[:, rows_at(sp, wide)] = dn_ref[u]

    with jax.named_scope("prep_q"):
        for h in range(heads):
            columns = slice(h * HEAD_SIZE, (h + 1) * HEAD_SIZE)

            @pl.loop(0, rows // GRID)
            def _(i):
                at, turned = turn(q_in, q_gain, columns, i)
                q_ref[at, columns] = turned

        top_s[...] = jnp.full(top_s.shape, -1e30, F32)
        sum_s[...] = jnp.zeros(sum_s.shape, F32)
        acc_s[...] = jnp.zeros(acc_s.shape, F32)
    factor = HEAD_SIZE ** (-0.5) * 1.4426950408889634

    def attend(owner):
        at = rows_at(owner, rows)
        with jax.named_scope("attend"):
            vt[...] = kvs[at, HEAD_SIZE:].astype(F32).T.astype(BF16)

            @pl.loop(0, tiles)
            def _(i):
                for h in range(heads):
                    q = q_ref[rows_at(i, tile), h * HEAD_SIZE : (h + 1) * HEAD_SIZE]
                    s = lax.dot_general(
                        kvs[at, 0:HEAD_SIZE], q, (((1,), (1,)), ((), ())),
                        preferred_element_type=F32,
                    )
                    n = i * heads + h
                    top = top_s[n]
                    new_top = jnp.maximum(top, jnp.max(s, axis=0, keepdims=True))
                    fade = jnp.exp2((top - new_top) * factor)
                    w = jnp.exp2((s - new_top) * factor)
                    top_s[n] = new_top
                    sum_s[n] = sum_s[n] * fade + jnp.sum(w, axis=0, keepdims=True)
                    acc_s[n] = acc_s[n] * fade + jnp.dot(
                        vt[...], w.astype(BF16), preferred_element_type=F32
                    )

    kc = {}

    def to_core(k, row, slot):
        at = spot(z_from[k] * 2 + row, c)
        kc[slot] = send(at, at, s_c, r_c, slot, core_peer)

    def near_arrived(k):
        got("kz", kz[k])
        at = spot(z_from[k] * 2 + y, c)
        ky.append(send(at, at, s_y, r_y, k, y_peer))
        to_core(k, y, 2 * k - 1)

    def far_arrived(k):
        got("ky", ky[k])
        to_core(k, 1 - y, 2 * k)

    def use(slot, owner):
        got("kc", kc[slot])
        attend(owner)

    order = [1] if nz == 2 else list(range(1, nz))
    attend(sp)
    far_arrived(0)
    near_arrived(1)
    use(0, z * 2 + 1 - y)
    gz, gy = {}, {}
    for k in range(1, nz):
        if k + 1 < nz:
            near_arrived(k + 1)
        else:
            far_arrived(1)
        if k + 1 == nz - 1 or nz == 2:
            with jax.named_scope("w_kzs"):
                for i in range(1, nz):
                    kz[i].wait_send()
            for i in order:
                gz[i] = send(gu_ref.at[lax.rem(z_at[i], 2)], gu_all.at[rows_at(sp, depth), :],
                             s_gz, r_gz, i - 1, z_peers[i - 1])
        use(2 * k - 1, z_from[k] * 2 + y)
    gy[0] = send(gu_ref.at[u], gu_all.at[rows_at(sp, depth), :], s_gy, r_gy, 0, y_peer)
    for k in range(1, nz):
        if k + 1 < nz:
            far_arrived(k + 1)
        use(2 * k, z_from[k] * 2 + 1 - y)

    def cols(t):
        return rows_at(t, own)

    with jax.named_scope("proj"):
        @pl.loop(0, tiles)
        def _(i):
            parts = [
                (acc_s[i * heads + h] / sum_s[i * heads + h]).astype(BF16) for h in range(heads)
            ]
            whole = jnp.concatenate(parts, axis=0) if heads > 1 else parts[0]
            proj[rows_at(i, tile), :] = lax.dot_general(
                whole, w_ref[...], (((0,), (0,)), ((), ())), preferred_element_type=F32
            ).astype(BF16)

    step = rows // 8
    near = [
        send(proj.at[:, cols(xs[j] * 2 + 1 - c)], from_core.at[j], s1, r1, j, core_peer)
        for j in list(range(1, nx)) + [0]
    ]
    near = [near[-1]] + near[:-1]
    to_x = []
    for j in range(1, nx):
        got("near", near[j])

        @pl.loop(0, 8)
        def _(i):
            at = rows_at(i, step)
            outgo[j - 1, at, :] = (
                proj[at, cols(xs[j] * 2 + c)].astype(F32) + from_core[j, at, :].astype(F32)
            ).astype(BF16)

        to_x.append(send(outgo.at[j - 1], from_x.at[j - 1], s2, r2, j - 1, row_peers[j - 1]))
    got("near0", near[0])

    def relay_gu(k):
        got("gz", gz[k])
        at = gu_all.at[rows_at(z_from[k] * 2 + y, depth), :]
        gy[k] = send(at, at, s_gy, r_gy, k, y_peer)

    relay_gu(order[0])
    dy = {0: send(dn_ref.at[u], dn_all.at[:, rows_at(sp, wide)], s_dy, r_dy, 0, y_peer)}

    for copy in to_x:
        got("tox", copy)
    ones = jnp.ones((8, own), F32)

    with jax.named_scope("mid"):
        for i in range(tiles):
            at = pl.ds(i * tile, tile)
            total = proj[at, cols(tp)].astype(F32) + from_core[0, at, :].astype(F32)
            for j in range(1, nx):
                total += from_x[j - 1, at, :].astype(F32)
            mid = res_ref[at, :].astype(F32) + total
            mid_ref[at, :] = mid
            squares[0, :, at] = lax.dot_general(
                ones, mid * mid, (((1,), (1,)), ((), ())),
                precision=lax.Precision.HIGHEST, preferred_element_type=F32,
            )
    peers = [core_peer] + row_peers + across
    sq = [send(squares.at[0], squares.at[k + 1], s3, r3, k, peers[k]) for k in range(len(peers))]
    for copy in sq:
        got("sq", copy)

    def home(uu, t):
        return normed_ref.at[rows_at(uu, rows), cols(t)]

    with jax.named_scope("norm"):
        for i in range(tiles):
            at = pl.ds(i * tile, tile)
            square = squares[0, :, at]
            for k in range(len(peers)):
                square += squares[k + 1, :, at]
            scale = lax.rsqrt(square.T[:, 0:1] / (n_tp * own) + eps)
            block[at, :] = (mid_ref[at, :] * scale * gain_ref[:, cols(tp)]).astype(BF16)
    az = send(block, home(u, tp), s_az, r_az, 0, z_pair)
    ax = [send(block, home(u, tp), s_ax, r_ax, j - 1, row_peers[j - 1]) for j in range(1, nx)]
    ac = [send(block, home(u, tp), s_ac, r_ac, 0, core_peer)]
    normed_ref[rows_at(u, rows), cols(tp)] = block[...]

    def on_core(uu, t, slot):
        at = home(uu, t)
        ac.append(send(at, at, s_ac, r_ac, slot, core_peer))

    for k in order[1:2]:
        relay_gu(k)
    for j in range(1, nx):
        got("ax", ax[j - 1])
        on_core(u, back[j] * 2 + c, j)
    got("az", az)
    there = home(1 - u, tp)
    ar = [send(there, there, s_ar, r_ar, j - 1, row_peers[j - 1]) for j in range(1, nx)]
    on_core(1 - u, tp, nx)
    dz = {
        k: send(dn_ref.at[lax.rem(z_at[k], 2)], dn_all.at[:, rows_at(sp, wide)],
                s_dz, r_dz, k - 1, z_peers[k - 1])
        for k in order
    }
    for k in order[2:]:
        relay_gu(k)

    def gate_up(owner, first=False):
        ks = rows_at(owner, depth)
        with jax.named_scope("gate_up"):
            @pl.loop(0, 2 * rows // 384)
            def _(i):
                at = rows_at(i, 384)
                term = jnp.dot(normed_ref[at, ks], gu_all[ks, :], preferred_element_type=F32)
                gu_acc[at, :] = term if first else gu_acc[at, :] + term

    def relay_dn(k):
        got("dz", dz[k])
        at = dn_all.at[:, rows_at(z_from[k] * 2 + y, wide)]
        dy[k] = send(at, at, s_dy, r_dy, k, y_peer)

    for j in range(1, nx):
        got("ar", ar[j - 1])
        on_core(1 - u, back[j] * 2 + c, nx + j)
    for copy in ac:
        got("ac", copy)
    gate_up(sp, True)
    for k in order:
        gate_up(z_from[k] * 2 + y)
    for k in [0] + order:
        got("gy", gy[k])
        gate_up(z_from[k] * 2 + 1 - y)
        if k > 0:
            relay_dn(k)

    with jax.named_scope("hidden"):
        @pl.loop(0, 2 * rows // 128)
        def _(i):
            at = rows_at(i, 128)
            gate = gu_acc[at, :units]
            hidden[at, :] = (gate / (1.0 + jnp.exp(-gate)) * gu_acc[at, units:]).astype(BF16)

    def down(owner):
        ks = rows_at(owner, wide)
        with jax.named_scope("down"):
            @pl.loop(0, 2 * rows // 384)
            def _(i):
                at = rows_at(i, 384)
                terms[at, ks] = jnp.dot(
                    hidden[at, :], dn_all[:, ks], preferred_element_type=F32
                ).astype(BF16)

    down(sp)
    for k in order:
        down(z_from[k] * 2 + y)
    for k in [0] + order:
        got("dy", dy[k])
        down(z_from[k] * 2 + 1 - y)

    top, low = pl.ds(0, half), pl.ds(half, half)
    x_peers = [(sp, xs[j] * 2 + c) for j in range(nx)]
    every = [(1 - u, xs[j]) for j in range(nx)] + [(u, xs[j]) for j in range(1, nx)] + [(u, x)]
    turns = list(range(1, 2 * nx - 1)) + [0, 2 * nx - 1]
    side = {}
    for k in turns:
        uu, xx = every[k]
        side[k] = send(terms.at[rows_at(uu, rows), cols(xx * 2 + 1 - c)], d_core.at[k],
                       e1, f1, k, core_peer)
    to_z, to_x, again = {}, {}, []
    for k in turns[:-1]:
        uu, xx = every[k]
        got("side", side[k])

        @pl.loop(0, 8)
        def _(i):
            at = rows_at(i, step)
            here = pl.ds(pl.multiple_of(uu * rows + i * step, step), step)
            d_out[k, at, :] = (
                terms[here, cols(xx * 2 + c)].astype(F32) + d_core[k, at, :].astype(F32)
            ).astype(BF16)

        if k < nx:
            to_z[k] = send(d_out.at[k, top], d_y.at[k], e2, f2, k, z_pair)
        j = k if k < nx else k - nx + 1
        if j > 0:
            slot = 2 * (j - 1) + (1 if k < nx else 0)
            to_x[slot] = send(d_out.at[k, low], d_x.at[slot], e3, f3, slot, x_peers[j])
    for j in range(1, nx):
        got("to_z", to_z[j])

        @pl.loop(0, 4)
        def _(i):
            at = rows_at(i, step)
            relay[j, at, :] = (
                d_out[nx + j - 1, at, :].astype(F32) + d_y[j, at, :].astype(F32)
            ).astype(BF16)

        again.append(send(relay.at[j], last_x.at[j - 1], e4, f4, j - 1, x_peers[j]))
    for j in range(1, nx):
        got("to_x", to_x[2 * j - 1])

    @pl.loop(0, 4)
    def _(i):
        at = rows_at(i, step)
        here = pl.ds(pl.multiple_of(half + i * step, step), step)
        total = d_out[0, here, :].astype(F32)
        for j in range(1, nx):
            total += d_x[2 * j - 1, at, :].astype(F32)
        relay[0, at, :] = total.astype(BF16)

    again.append(send(relay.at[0], last_y, e5, f5, 0, z_pair))
    got("side", side[2 * nx - 1])
    got("to_z", to_z[0])
    for j in range(1, nx):
        got("to_x", to_x[2 * j - 2])
    for copy in again:
        got("again", copy)

    with jax.named_scope("final"):
        @pl.loop(0, 4)
        def _(i):
            at = rows_at(i, step)
            for part in range(2):
                to = pl.ds(pl.multiple_of(part * half + i * step, step), step)
                here = pl.ds(pl.multiple_of(u * rows + part * half + i * step, step), step)
                total = terms[here, cols(tp)].astype(F32)
                total += d_core[2 * nx - 1, to, :].astype(F32)
                total += (d_y[0, at, :] if part == 0 else last_y[at, :]).astype(F32)
                for j in range(1, nx):
                    total += (last_x[j - 1, at, :] if part == 0
                              else d_x[2 * j - 2, at, :]).astype(F32)
                out_ref[to, :] = (mid_ref[to, :] + 0.5 * total).astype(BF16)

    kz_sends = {id(kz[i]) for i in range(1, nz)}
    with jax.named_scope("w_sends"):
        for copy in sends:
            if id(copy) not in kz_sends:
                copy.wait_send()


def layer(q, k, v, q_gain, k_gain, w, res, gain, gate, up, dn, n_sp, n_tp):
    nz, nx = n_sp // 2, n_tp // 2
    rows, own = res.shape
    heads = q.shape[1] // HEAD_SIZE
    tile = 256 if rows % 256 == 0 else rows
    count = heads * (rows // tile)
    width = n_tp * own
    depth, twice = gate.shape
    wide = dn.shape[2]
    dma = pltpu.SemaphoreType.DMA
    n = 2 * nx
    vm = pl.BlockSpec(memory_space=pltpu.VMEM)

    def two(k):
        return [dma((k,)), dma((k,))]

    def bf(*shape):
        return pltpu.VMEM(shape, BF16)

    def fl(*shape):
        return pltpu.VMEM(shape, F32)

    return pl.pallas_call(
        functools.partial(layer_kernel, nz, nx, heads),
        out_shape=jax.ShapeDtypeStruct((rows, own), BF16),
        in_specs=[vm] * 15,
        out_specs=vm,
        scratch_shapes=[
            bf(rows, heads * HEAD_SIZE), bf(rows, 2 * HEAD_SIZE),
            bf(n_sp * rows, 2 * HEAD_SIZE), bf(HEAD_SIZE, rows),
            fl(count, 1, tile), fl(count, 1, tile), fl(count, HEAD_SIZE, tile),
            bf(rows, width), bf(nx, rows, own), bf(nx - 1, rows, own), bf(nx - 1, rows, own),
            fl(n, 8, rows), bf(rows, own), fl(rows, own), bf(2 * rows, width),
            bf(2, depth, twice), bf(n_sp * depth, twice), bf(dn.shape[1], n_sp * wide),
            fl(2 * rows, twice), bf(2 * rows, twice // 2), bf(2 * rows, width),
            bf(n, rows, own), bf(n - 1, rows, own), bf(nx, rows // 2, own),
            bf(n - 2, rows // 2, own), bf(nx, rows // 2, own), bf(nx - 1, rows // 2, own),
            bf(rows // 2, own),
        ] + two(nz - 1) + two(nz) + two(2 * nz - 1) + two(nx) + two(nx - 1) + two(n - 1)
        + two(nx - 1) + two(1) + two(nx - 1) + two(2 * nx)
        + two(nz - 1) + two(nz) + two(nz - 1) + two(nz)
        + two(n) + two(nx) + two(n - 2) + two(nx - 1) + two(1),
        compiler_params=pltpu.CompilerParams(
            collective_id=0, has_side_effects=True, vmem_limit_bytes=VMEM_LIMIT
        ),
        name="layer",
    )(q, k, v, q_gain, k_gain, w, res, gain, gate, up, dn, *rotary_tables(n_sp * rows))


def on_device(n_sp, n_tp, residual_in, queries, keys, values, query_gain, key_norm_gain,
              out_weight, mlp_gain, gate_weight, up_weight, down_weight):
    down = down_weight.reshape(2, down_weight.shape[0] // 2, down_weight.shape[1])
    return layer(
        queries, keys, values, query_gain[None, :], key_norm_gain[None, :], out_weight,
        residual_in, mlp_gain[None, :], gate_weight, up_weight, down, n_sp, n_tp,
    )


def solution(mesh):
    in_specs = (
        P("sp", "tp"),
        P("sp", "tp"),
        P("sp", None),
        P("sp", None),
        P(),
        P(),
        P("tp", None),
        P(),
        P("sp", "tp"),
        P("sp", "tp"),
        P("tp", "sp"),
    )
    out_specs = P("sp", "tp")
    return jax.shard_map(
        functools.partial(on_device, mesh.shape["sp"], mesh.shape["tp"]),
        mesh=mesh, in_specs=in_specs, out_specs=out_specs, check_vma=False,
    )
```

```python
import functools
import jax
import numpy as np
import jax.numpy as jnp
from jax import lax
from jax.experimental import pallas as pl
from jax.experimental.pallas import tpu as pltpu
from jax.sharding import PartitionSpec as P

D = 2048
HEAD_SIZE = 128
QUERY_HEADS = 8
KEY_VALUE_HEADS = 2
GRID = 64

eps = 1e-06
rotary_base = 10000.0
MESH = pl.DeviceIdType.MESH
VMEM_LIMIT = 67043328
F32 = jnp.float32
BF16 = jnp.bfloat16


def remote(src, dst, send, recv, sp, tp):
    copy = pltpu.make_async_remote_copy(
        src_ref=src, dst_ref=dst, send_sem=send, recv_sem=recv,
        device_id={"sp": sp, "tp": tp}, device_id_type=MESH,
    )
    copy.start()
    return copy


def greet(peers):
    barrier = pltpu.get_barrier_semaphore()
    for sp, tp in peers:
        pl.semaphore_signal(
            barrier, inc=1, device_id={"sp": sp, "tp": tp}, device_id_type=MESH
        )
    pl.semaphore_wait(barrier, len(peers))


def place():
    sp = lax.axis_index("sp")
    tp = lax.axis_index("tp")
    return sp, tp, sp // 2, lax.rem(sp, 2), tp // 2, lax.rem(tp, 2)


def rows_at(index, size):
    return pl.ds(pl.multiple_of(index * size, size), size)


def rotary_tables(tokens):
    half_size = HEAD_SIZE // 2
    frequency = np.float32(rotary_base) ** (
        -np.arange(0, half_size, 2, dtype=np.float32) / np.float32(half_size)
    )
    longest = max(tokens // GRID, GRID)
    angles = np.arange(longest, dtype=np.float32)[:, None] * frequency.astype(np.float32)
    cosine, sine = np.cos(angles), np.sin(angles)
    none = np.zeros_like(angles)
    rows = tokens // GRID
    pieces = [
        np.concatenate([cosine, none, cosine, none], axis=1)[:rows],
        np.concatenate([none, cosine, none, cosine], axis=1)[:GRID],
        np.concatenate([-sine, none, sine, none], axis=1)[:rows],
        np.concatenate([none, -sine, none, sine], axis=1)[:GRID],
    ]
    return [jnp.asarray(piece, F32) for piece in pieces]


def layer_kernel(nz, nx, heads, q_in, k_in, v_in, q_gain, k_gain, w_ref, res_ref, gain_ref,
                 gate_ref, up_ref, dn_ref, cos_row, cos_col, sin_row, sin_col,
                 out_ref,
                 q_ref, kv_ref, kvs, vt, top_s, sum_s, acc_s, proj, from_core, outgo, from_x,
                 squares, block, mid_ref, normed_ref, gu_ref, gu_all, dn_all, gu_acc, hidden,
                 ratio, column, terms, d_core, d_out, d_y, d_x, relay, last_x, last_y,
                 s_z, r_z, s_f, s_y, r_y, s_c, r_c, s1, r1, s2, r2, s3, r3,
                 s_ax, r_ax, s_az, r_az, s_ar, r_ar, s_ac, r_ac,
                 s_rz, r_rz, s_gz, r_gz, s_gy, r_gy, s_dz, r_dz, s_dy, r_dy,
                 e1, f1, e2, f2, e3, f3, e4, f4, e5, f5):
    sp, tp, z, y, x, c = place()
    rows, own = res_ref.shape
    n_tp = 2 * nx
    half = rows // 2
    tile = 256 if rows % 256 == 0 else rows
    tiles = rows // tile
    depth, twice = gate_ref.shape
    units = twice // 2
    wide = dn_ref.shape[2]
    other = x * 2 + 1 - c
    u = lax.rem(z, 2)
    z_other = z + 1 - 2 * u
    nh = nz // 2
    inner = lax.rem(z // 2 + u, 2)
    flip = lax.rem(u + inner, 2)
    z_to, z_from, slots_z = [z_other], [z_other], [0]
    for d in range(1, nh):
        ahead = lax.rem(z // 2 + d, nh) * 2
        behind = lax.rem(z // 2 - d + nh, nh) * 2
        z_to += [ahead + flip, ahead + 1 - flip]
        z_from += [behind + flip, behind + 1 - flip]
        slots_z += [2 * d - 1 + inner, 2 * d - inner]
    xs = [lax.rem(x + j, nx) for j in range(nx)]
    back = [lax.rem(x - j + nx, nx) for j in range(nx)]
    y_peer = (z * 2 + 1 - y, tp)
    core_peer = (sp, other)
    z_pair = (z_other * 2 + y, tp)
    z_peers = [(k * 2 + y, tp) for k in z_to]
    far = range(nz - 1)
    row_peers = [(sp, xs[j] * 2 + c) for j in range(1, nx)]
    across = [(sp, xs[j] * 2 + 1 - c) for j in range(1, nx)]

    def turn(ref, gain, columns, i):
        at = rows_at(i, GRID)
        v = ref[at, columns].astype(F32)
        v = v * lax.rsqrt(jnp.mean(v * v, axis=1, keepdims=True) + eps) * gain[...]
        row = sp * (rows // GRID) + i
        cosine = cos_row[pl.ds(row, 1), :] + cos_col[...]
        sine = sin_row[pl.ds(row, 1), :] + sin_col[...]
        return at, (v * cosine + pltpu.roll(v, HEAD_SIZE // 2, 1) * sine).astype(BF16)

    barrier = pltpu.get_barrier_semaphore()
    friends = z_peers + [y_peer, core_peer] + row_peers + across
    for to_sp, to_tp in friends:
        pl.semaphore_signal(
            barrier, inc=1, device_id={"sp": to_sp, "tp": to_tp}, device_id_type=MESH
        )

    with jax.named_scope("prep"):
        shared = pl.ds(
            pl.multiple_of(tp * heads // (QUERY_HEADS // KEY_VALUE_HEADS) * HEAD_SIZE, HEAD_SIZE),
            HEAD_SIZE,
        )

        @pl.loop(0, rows // GRID, unroll=4)
        def _(i):
            at, turned = turn(k_in, k_gain, shared, i)
            kv_ref[at, 0:HEAD_SIZE] = turned
            kv_ref[at, HEAD_SIZE:] = v_in[at, shared]

        for part in range(2):
            cut = slice(part * units, (part + 1) * units)
            for i in range(0, depth, 64):
                gu_ref[part, i : i + 64, :] = jnp.concatenate(
                    [gate_ref[i : i + 64, cut].astype(F32), up_ref[i : i + 64, cut].astype(F32)],
                    axis=1,
                ).astype(BF16)

    with jax.named_scope("greet"):
        pl.semaphore_wait(barrier, len(friends))

    def spot(owner, side):
        return kvs.at[pl.ds(pl.multiple_of(owner * rows + side * half, half), half), :]

    sends = []

    def describe(src, dst, out, arrive, slot, to):
        copy = pltpu.make_async_remote_copy(
            src_ref=src, dst_ref=dst, send_sem=out.at[slot], recv_sem=arrive.at[slot],
            device_id={"sp": to[0], "tp": to[1]}, device_id_type=MESH,
        )
        sends.append(copy)
        return copy

    def send(src, dst, out, arrive, slot, to):
        copy = remote(src, dst, out.at[slot], arrive.at[slot], *to)
        sends.append(copy)
        return copy

    def got(name, copy):
        with jax.named_scope("w_" + name):
            copy.wait_recv()

    mine = kv_ref.at[rows_at(c, half), :]
    send(mine, spot(sp, c), s_z, r_z, 0, z_pair)
    key_from = [(z_other, 0)]
    for d in range(1, nh):
        ahead = lax.rem(z // 2 + d, nh)
        behind = lax.rem(z // 2 - d + nh, nh)
        target = ((ahead * 2 + lax.rem(ahead + 1, 2)) * 2 + y, tp)
        send(mine, spot(sp, c), s_z, r_z, 2 * d - 1 + u, target)
        key_from += [(behind * 2 + uu, 2 * d - 1 + uu) for uu in range(2)]
    passed = []
    ky = [send(mine, spot(sp, c), s_y, r_y, 0, y_peer)]
    gz, gy, dz, dy = {}, {}, {}, {}

    def pieces(k):
        return 1 if k <= 0 else 2

    def gu_at(owner, k, a):
        size = depth // pieces(k)
        return gu_all.at[pl.ds(pl.multiple_of(owner * depth + a * size, size), size), :]

    def give_gu(k):
        for a in range(pieces(k)):
            size = depth // pieces(k)
            gz[k, a] = describe(gu_ref.at[lax.rem(z_to[k], 2), pl.ds(a * size, size)],
                                gu_at(sp, k, a), s_gz, r_gz, slots_z[k] * 2 + a, z_peers[k])

    def give_dn(k):
        dz[k] = describe(dn_ref.at[lax.rem(z_to[k], 2)], dn_all.at[:, rows_at(sp, wide)],
                         s_dz, r_dz, slots_z[k], z_peers[k])

    dy[-1] = send(dn_ref.at[u], dn_all.at[:, rows_at(sp, wide)], s_dy, r_dy, 0, y_peer)
    for k in far:
        give_gu(k)
        give_dn(k)

    def give_pair():
        gz[0, 0].start()

    pl.when(inner == 0)(give_pair)
    dz[0].start()
    for k in far[1:]:
        for a in range(pieces(k)):
            gz[k, a].start()
    kvs[rows_at(sp, rows), :] = kv_ref[...]
    gu_all[rows_at(sp, depth), :] = gu_ref[u]
    dn_all[:, rows_at(sp, wide)] = dn_ref[u]

    with jax.named_scope("prep_q"):
        for h in range(heads):
            columns = slice(h * HEAD_SIZE, (h + 1) * HEAD_SIZE)

            @pl.loop(0, rows // GRID, unroll=4)
            def _(i):
                at, turned = turn(q_in, q_gain, columns, i)
                q_ref[at, columns] = turned

        top_s[...] = jnp.full(top_s.shape, -1e30, F32)
        sum_s[...] = jnp.zeros(sum_s.shape, F32)
        acc_s[...] = jnp.zeros(acc_s.shape, F32)
    factor = HEAD_SIZE ** (-0.5) * 1.4426950408889634

    def turn_values(owner):
        vt[owner] = kvs[rows_at(owner, rows), HEAD_SIZE:].astype(F32).T.astype(BF16)

    def attend(owner, start, stop):
        at = rows_at(owner, rows)
        with jax.named_scope("attend"):

            @pl.loop(start, stop)
            def _(i):
                slots = [i * heads + h for h in range(heads)]
                states = [(top_s[n], sum_s[n], acc_s[n]) for n in slots]
                scores = [
                    lax.dot_general(
                        kvs[at, 0:HEAD_SIZE],
                        q_ref[rows_at(i, tile), h * HEAD_SIZE : (h + 1) * HEAD_SIZE],
                        (((1,), (1,)), ((), ())), preferred_element_type=F32,
                    )
                    for h in range(heads)
                ]
                values = vt[owner]
                for n, s, (top, total, acc) in zip(slots, scores, states):
                    new_top = jnp.maximum(top, jnp.max(s, axis=0, keepdims=True))
                    fade = jnp.exp2((top - new_top) * factor)
                    w = jnp.exp2((s - new_top) * factor)
                    top_s[n] = new_top
                    sum_s[n] = total * fade + jnp.sum(w, axis=0, keepdims=True)
                    acc_s[n] = acc * fade + jnp.dot(
                        values, w.astype(BF16), preferred_element_type=F32
                    )

    kc = {}
    first = max(tiles - 1, 1)

    def to_core(at, slot):
        kc[slot] = send(at, at, s_c, r_c, slot, core_peer)

    def near_arrived(k):
        plane, slot = key_from[k]
        at = spot(plane * 2 + y, c)
        copy = pltpu.make_async_remote_copy(
            src_ref=at, dst_ref=at, send_sem=s_f.at[slot], recv_sem=r_z.at[slot],
            device_id={"sp": z_pair[0], "tp": tp}, device_id_type=MESH,
        )
        got("kz", copy)
        if k > 0:
            passed.append(copy)

            @pl.when(inner == 1)
            def _():
                copy.start()

        ky.append(send(at, at, s_y, r_y, k + 1, y_peer))
        to_core(at, 2 * k + 1)

    def far_arrived(k):
        got("ky", ky[k])
        to_core(spot((z if k == 0 else key_from[k - 1][0]) * 2 + 1 - y, c), 2 * k)

    def use(slot, owner):
        got("kc", kc[slot])
        turn_values(owner)
        attend(owner, 0, first)

    turn_values(sp)
    attend(sp, 0, first)
    far_arrived(0)
    near_arrived(0)
    use(0, z * 2 + 1 - y)
    for k in far:
        if k + 1 in far:
            near_arrived(k + 1)
        else:
            far_arrived(1)
        if k == far[-2]:
            pl.when(inner == 1)(give_pair)
            gy[-1, 0] = send(gu_ref.at[u], gu_all.at[rows_at(sp, depth), :], s_gy, r_gy, 0, y_peer)
        use(2 * k + 1, key_from[k][0] * 2 + y)
    for k in far:
        if k + 1 in far:
            far_arrived(k + 2)
        use(2 * k + 2, key_from[k][0] * 2 + 1 - y)

    def cols(t):
        return rows_at(t, own)

    def project(i):
        with jax.named_scope("proj"):
            parts = [
                (acc_s[i * heads + h] / sum_s[i * heads + h]).astype(BF16) for h in range(heads)
            ]
            whole = jnp.concatenate(parts, axis=0) if heads > 1 else parts[0]
            proj[rows_at(i, tile), :] = lax.dot_general(
                whole, w_ref[...], (((0,), (0,)), ((), ())), preferred_element_type=F32
            ).astype(BF16)

    near, to_x = {}, {}
    step = rows // 8
    small = tile // 4

    def give_core(t):
        at = pl.ds(t * tile, tile)
        for j in list(range(1, nx)) + [0]:
            near[t, j] = send(proj.at[at, cols(xs[j] * 2 + 1 - c)], from_core.at[j, at],
                              s1, r1, t * nx + j, core_peer)

    def give_x(t):
        for j in range(1, nx):
            got("near", near[t, j])

            @pl.loop(0, 4)
            def _(i):
                at = pl.ds(pl.multiple_of(t * tile + i * small, small), small)
                outgo[j - 1, at, :] = (
                    proj[at, cols(xs[j] * 2 + c)].astype(F32) + from_core[j, at, :].astype(F32)
                ).astype(BF16)

            at = pl.ds(t * tile, tile)
            to_x[t, j] = send(outgo.at[j - 1, at], from_x.at[j - 1, at], s2, r2,
                              t * (nx - 1) + j - 1, row_peers[j - 1])
        got("near", near[t, 0])

    def later(begin, end):
        @pl.loop(begin, end)
        def _(b):
            attend(b, first, tiles)

    def relay_gu(k, a, condition=None):
        at = gu_at(z_from[k] * 2 + y, k, a)
        if (k, a) not in gy:
            slot = (k + 1) * 2 + a
            gy[k, a] = pltpu.make_async_remote_copy(
                src_ref=at, dst_ref=at, send_sem=s_gy.at[slot], recv_sem=r_gy.at[slot],
                device_id={"sp": y_peer[0], "tp": y_peer[1]}, device_id_type=MESH,
            )
            sends.append(gy[k, a])

        def pass_on():
            got("gz" + str(k) + str(a), gz[k, a])
            gy[k, a].start()

        if condition is None:
            pass_on()
        else:
            pl.when(condition)(pass_on)

    def have_gu(k):
        for a in range(pieces(k)):
            got("gy" + str(k), gy[k, a])

    def relay_dn(k, condition=None):
        at = dn_all.at[:, rows_at(z_from[k] * 2 + y, wide)]
        if k not in dy:
            dy[k] = describe(at, at, s_dy, r_dy, k + 1, y_peer)

        def pass_on():
            got("dz" + str(k), dz[k])
            dy[k].start()

        if condition is None:
            pass_on()
        else:
            pl.when(condition)(pass_on)

    for t in range(first):
        project(t)
        give_core(t)
    relay_gu(0, 0, inner == 1)
    if tiles > first:
        later(0, 2)
    for t in range(first):
        give_x(t)
    for t in range(first, tiles):
        later(2, 2 * nz)
        project(t)
        give_core(t)
    relay_dn(0, inner == 1)
    relay_gu(0, 0, inner == 0)
    for t in range(first, tiles):
        give_x(t)

    ones = jnp.ones((8, own), F32)
    peers = [core_peer] + row_peers + across
    az, ax, ac, ar = [], {}, {}, {}

    def home(uu, tt, t):
        return normed_ref.at[rows_at(uu * tiles + t, tile), cols(tt)]

    def on_core(uu, tt, t, slot):
        at = home(uu, tt, t)
        ac[t, slot] = send(at, at, s_ac, r_ac, t * 2 * nx + slot, core_peer)

    def add_up(t):
        for j in range(1, nx):
            got("tox", to_x[t, j])
        at = pl.ds(t * tile, tile)
        with jax.named_scope("mid"):
            total = proj[at, cols(tp)].astype(F32) + from_core[0, at, :].astype(F32)
            for j in range(1, nx):
                total += from_x[j - 1, at, :].astype(F32)
            mid = res_ref[at, :].astype(F32) + total
            mid_ref[at, :] = mid
            made = (mid * gain_ref[:, cols(tp)]).astype(BF16)
            block[at, :] = made
            normed_ref[rows_at(u * tiles + t, tile), cols(tp)] = made
            squares[0, :, at] = lax.dot_general(
                ones, mid * mid, (((1,), (1,)), ((), ())),
                precision=lax.Precision.HIGHEST, preferred_element_type=F32,
            )
        az.append(send(block.at[at], home(u, tp, t), s_az, r_az, t, z_pair))
        for j in range(1, nx):
            ax[t, j] = send(block.at[at], home(u, tp, t), s_ax, r_ax, t * (nx - 1) + j - 1,
                            row_peers[j - 1])
        ac[t, 0] = send(block.at[at], home(u, tp, t), s_ac, r_ac, t * 2 * nx, core_peer)

    for t in range(tiles):
        add_up(t)
        if t == 0:
            for k in far[1:2]:
                relay_gu(k, 0, inner == 1)
    sq = [send(squares.at[0], squares.at[k + 1], s3, r3, k, peers[k]) for k in range(len(peers))]
    for k in far[1:]:
        dz[k].start()
    def gate_up(plane, uu, fresh=False):
        ks = rows_at(plane, 2 * depth)
        with jax.named_scope("gate_up"):
            @pl.loop(0, rows // 384)
            def _(i):
                at = pl.ds(pl.multiple_of(uu * rows + i * 384, 384), 384)
                term = jnp.dot(normed_ref[at, ks], gu_all[ks, :], preferred_element_type=F32)
                gu_acc[at, :] = term if fresh else gu_acc[at, :] + term

    for t in range(tiles):
        for j in range(1, nx):
            got("ax", ax[t, j])
            on_core(u, back[j] * 2 + c, t, j)
    for t in range(tiles):
        for j in range(nx):
            got("ac", ac[t, j])
    for k in far[1:2]:
        relay_gu(k, 0, inner == 0)
    relay_dn(0, inner == 0)
    have_gu(-1)
    gate_up(z, u, True)
    for k in far[1:2]:
        relay_gu(k, 1)
    have_gu(0)
    gate_up(z_from[0], u)
    for k in far[2:3]:
        relay_gu(k, 0)
    for t in range(tiles):
        if t == tiles - 1:
            for k in far[2:3]:
                relay_gu(k, 1)
        got("az", az[t])
        there = home(1 - u, tp, t)
        for j in range(1, nx):
            ar[t, j] = send(there, there, s_ar, r_ar, t * (nx - 1) + j - 1, row_peers[j - 1])
        on_core(1 - u, tp, t, nx)
    for copy in sq:
        got("sq", copy)
    with jax.named_scope("norm"):
        square = squares[0]
        for k in range(len(peers)):
            square += squares[k + 1]
        ratio[u] = lax.rsqrt(square / (n_tp * own) + eps)
    ratio_z = send(ratio.at[u], ratio.at[u], s_rz, r_rz, 0, z_pair)
    for k in far[3:]:
        for a in range(2):
            relay_gu(k, a)
    for k in far[1:2]:
        relay_dn(k, inner == 0)
    for t in range(tiles):
        for j in range(1, nx):
            got("ar", ar[t, j])
            on_core(1 - u, back[j] * 2 + c, t, nx + j)
    for k in far[1:2]:
        relay_dn(k, inner == 1)
    for k in far[2:3]:
        relay_dn(k, inner == 0)
    for t in range(tiles):
        for j in range(nx, 2 * nx):
            got("ac", ac[t, j])
    gate_up(z, 1 - u, True)
    gate_up(z_from[0], 1 - u)
    for k in far[2:3]:
        relay_dn(k, inner == 1)
    for k in far[3:]:
        relay_dn(k)
    for k in far[1:]:
        have_gu(k)
        gate_up(z_from[k], 1 - u)
        gate_up(z_from[k], u)

    got("ratio", ratio_z)
    for uu in range(2):
        column[pl.ds(uu * rows, rows), :] = ratio[uu].T
    with jax.named_scope("hidden"):
        for uu in range(2):
            @pl.loop(0, rows // 128)
            def _(i):
                at = pl.ds(pl.multiple_of(uu * rows + i * 128, 128), 128)
                scale = column[at, 0:1]
                gate = gu_acc[at, :units] * scale
                hidden[at, :] = (
                    gate / (1.0 + jnp.exp(-gate)) * (gu_acc[at, units:] * scale)
                ).astype(BF16)

    for k in [-1] + list(far):
        got("dy", dy[k])
    top, low = pl.ds(0, half), pl.ds(half, half)
    x_peers = [(sp, xs[j] * 2 + c) for j in range(nx)]
    every = [(1 - u, xs[j]) for j in range(nx)] + [(u, xs[j]) for j in range(1, nx)] + [(u, x)]
    turns = list(range(1, 2 * nx - 1)) + [0, 2 * nx - 1]
    side, to_z, to_x, again = {}, {}, {}, []

    def down(k):
        uu, xx = every[k]
        ks = rows_at(xx, 2 * own)
        with jax.named_scope("down"):
            @pl.loop(0, rows // 384)
            def _(i):
                at = pl.ds(pl.multiple_of(uu * rows + i * 384, 384), 384)
                terms[at, ks] = jnp.dot(
                    hidden[at, :], dn_all[:, ks], preferred_element_type=F32
                ).astype(BF16)

        side[k] = send(terms.at[rows_at(uu, rows), cols(xx * 2 + 1 - c)], d_core.at[k],
                       e1, f1, k, core_peer)

    def forward(k):
        uu, xx = every[k]
        got("side", side[k])

        @pl.loop(0, 8)
        def _(i):
            at = rows_at(i, step)
            here = pl.ds(pl.multiple_of(uu * rows + i * step, step), step)
            d_out[k, at, :] = (
                terms[here, cols(xx * 2 + c)].astype(F32) + d_core[k, at, :].astype(F32)
            ).astype(BF16)

        if k < nx:
            to_z[k] = send(d_out.at[k, top], d_y.at[k], e2, f2, k, z_pair)
        j = k if k < nx else k - nx + 1
        if j > 0:
            slot = 2 * (j - 1) + (1 if k < nx else 0)
            to_x[slot] = send(d_out.at[k, low], d_x.at[slot], e3, f3, slot, x_peers[j])

    for i, k in enumerate(turns):
        down(k)
        if i > 0:
            forward(turns[i - 1])
    for j in range(1, nx):
        got("to_z", to_z[j])

        @pl.loop(0, 4)
        def _(i):
            at = rows_at(i, step)
            relay[j, at, :] = (
                d_out[nx + j - 1, at, :].astype(F32) + d_y[j, at, :].astype(F32)
            ).astype(BF16)

        again.append(send(relay.at[j], last_x.at[j - 1], e4, f4, j - 1, x_peers[j]))
    for j in range(1, nx):
        got("to_x", to_x[2 * j - 1])

    @pl.loop(0, 4)
    def _(i):
        at = rows_at(i, step)
        here = pl.ds(pl.multiple_of(half + i * step, step), step)
        total = d_out[0, here, :].astype(F32)
        for j in range(1, nx):
            total += d_x[2 * j - 1, at, :].astype(F32)
        relay[0, at, :] = total.astype(BF16)

    again.append(send(relay.at[0], last_y, e5, f5, 0, z_pair))
    got("side", side[2 * nx - 1])
    got("to_z", to_z[0])
    for j in range(1, nx):
        got("to_x", to_x[2 * j - 2])
    for copy in again:
        got("again", copy)

    with jax.named_scope("final"):
        @pl.loop(0, 4)
        def _(i):
            at = rows_at(i, step)
            for part in range(2):
                to = pl.ds(pl.multiple_of(part * half + i * step, step), step)
                here = pl.ds(pl.multiple_of(u * rows + part * half + i * step, step), step)
                total = terms[here, cols(tp)].astype(F32)
                total += d_core[2 * nx - 1, to, :].astype(F32)
                total += (d_y[0, at, :] if part == 0 else last_y[at, :]).astype(F32)
                for j in range(1, nx):
                    total += (last_x[j - 1, at, :] if part == 0
                              else d_x[2 * j - 2, at, :]).astype(F32)
                out_ref[to, :] = (mid_ref[to, :] + 0.5 * total).astype(BF16)

    with jax.named_scope("w_sends"):
        @pl.when(inner == 1)
        def _():
            for copy in passed:
                copy.wait_send()

        for copy in sends:
            copy.wait_send()


def layer(q, k, v, q_gain, k_gain, w, res, gain, gate, up, dn, n_sp, n_tp):
    nz, nx = n_sp // 2, n_tp // 2
    rows, own = res.shape
    heads = q.shape[1] // HEAD_SIZE
    tile = 256 if rows % 256 == 0 else rows
    tiles = rows // tile
    count = heads * tiles
    width = n_tp * own
    depth, twice = gate.shape
    wide = dn.shape[2]
    dma = pltpu.SemaphoreType.DMA
    n = 2 * nx
    vm = pl.BlockSpec(memory_space=pltpu.VMEM)

    def two(k):
        return [dma((k,)), dma((k,))]

    def bf(*shape):
        return pltpu.VMEM(shape, BF16)

    def fl(*shape):
        return pltpu.VMEM(shape, F32)

    return pl.pallas_call(
        functools.partial(layer_kernel, nz, nx, heads),
        out_shape=jax.ShapeDtypeStruct((rows, own), BF16),
        in_specs=[vm] * 15,
        out_specs=vm,
        scratch_shapes=[
            bf(rows, heads * HEAD_SIZE), bf(rows, 2 * HEAD_SIZE),
            bf(n_sp * rows, 2 * HEAD_SIZE), bf(n_sp, HEAD_SIZE, rows),
            fl(count, 1, tile), fl(count, 1, tile), fl(count, HEAD_SIZE, tile),
            bf(rows, width), bf(nx, rows, own), bf(nx - 1, rows, own), bf(nx - 1, rows, own),
            fl(n, 8, rows), bf(rows, own), fl(rows, own), bf(2 * rows, width),
            bf(2, depth, twice), bf(n_sp * depth, twice), bf(dn.shape[1], n_sp * wide),
            fl(2 * rows, twice), bf(2 * rows, twice // 2), fl(2, 8, rows), fl(2 * rows, 8), bf(2 * rows, width),
            bf(n, rows, own), bf(n - 1, rows, own), bf(nx, rows // 2, own),
            bf(n - 2, rows // 2, own), bf(nx, rows // 2, own), bf(nx - 1, rows // 2, own),
            bf(rows // 2, own),
        ] + two(nz - 1) + [dma((nz - 1,))] + two(nz) + two(2 * nz - 1)
        + two(tiles * nx) + two(tiles * (nx - 1)) + two(n - 1)
        + two(tiles * (nx - 1)) + two(tiles) + two(tiles * (nx - 1)) + two(tiles * 2 * nx)
        + two(1) + two(2 * nz) + two(2 * nz) + two(nz - 1) + two(nz)
        + two(n) + two(nx) + two(n - 2) + two(nx - 1) + two(1),
        compiler_params=pltpu.CompilerParams(
            collective_id=0, has_side_effects=True, vmem_limit_bytes=VMEM_LIMIT
        ),
        name="layer",
    )(q, k, v, q_gain, k_gain, w, res, gain, gate, up, dn, *rotary_tables(n_sp * rows))


def on_device(n_sp, n_tp, residual_in, queries, keys, values, query_gain, key_norm_gain,
              out_weight, mlp_gain, gate_weight, up_weight, down_weight):
    down = down_weight.reshape(2, down_weight.shape[0] // 2, down_weight.shape[1])
    return layer(
        queries, keys, values, query_gain[None, :], key_norm_gain[None, :], out_weight,
        residual_in, mlp_gain[None, :], gate_weight, up_weight, down, n_sp, n_tp,
    )


def solution(mesh):
    in_specs = (
        P("sp", "tp"),
        P("sp", "tp"),
        P("sp", None),
        P("sp", None),
        P(),
        P(),
        P("tp", None),
        P(),
        P("sp", "tp"),
        P("sp", "tp"),
        P("tp", "sp"),
    )
    out_specs = P("sp", "tp")
    return jax.shard_map(
        functools.partial(on_device, mesh.shape["sp"], mesh.shape["tp"]),
        mesh=mesh, in_specs=in_specs, out_specs=out_specs, check_vma=False,
    )
```

```python
import functools
import jax
import numpy as np
import jax.numpy as jnp
from jax import lax
from jax.experimental import pallas as pl
from jax.experimental.pallas import tpu as pltpu
from jax.sharding import PartitionSpec as P

D = 2048
HEAD_SIZE = 128
QUERY_HEADS = 8
KEY_VALUE_HEADS = 2
GRID = 64

eps = 1e-06
rotary_base = 10000.0
MESH = pl.DeviceIdType.MESH
VMEM_LIMIT = 67043328
F32 = jnp.float32
BF16 = jnp.bfloat16


def remote(src, dst, send, recv, sp, tp):
    copy = pltpu.make_async_remote_copy(
        src_ref=src, dst_ref=dst, send_sem=send, recv_sem=recv,
        device_id={"sp": sp, "tp": tp}, device_id_type=MESH,
    )
    copy.start()
    return copy


def greet(peers):
    barrier = pltpu.get_barrier_semaphore()
    for sp, tp in peers:
        pl.semaphore_signal(
            barrier, inc=1, device_id={"sp": sp, "tp": tp}, device_id_type=MESH
        )
    pl.semaphore_wait(barrier, len(peers))


def place():
    sp = lax.axis_index("sp")
    tp = lax.axis_index("tp")
    return sp, tp, sp // 2, lax.rem(sp, 2), tp // 2, lax.rem(tp, 2)


def rows_at(index, size):
    return pl.ds(pl.multiple_of(index * size, size), size)


def rotary_tables(tokens):
    half_size = HEAD_SIZE // 2
    frequency = np.float32(rotary_base) ** (
        -np.arange(0, half_size, 2, dtype=np.float32) / np.float32(half_size)
    )
    longest = max(tokens // GRID, GRID)
    angles = np.arange(longest, dtype=np.float32)[:, None] * frequency.astype(np.float32)
    cosine, sine = np.cos(angles), np.sin(angles)
    none = np.zeros_like(angles)
    rows = tokens // GRID
    pieces = [
        np.concatenate([cosine, none, cosine, none], axis=1)[:rows],
        np.concatenate([none, cosine, none, cosine], axis=1)[:GRID],
        np.concatenate([-sine, none, sine, none], axis=1)[:rows],
        np.concatenate([none, -sine, none, sine], axis=1)[:GRID],
    ]
    return [jnp.asarray(piece, F32) for piece in pieces]


def layer_kernel(nz, nx, heads, q_in, k_in, v_in, q_gain, k_gain, w_ref, res_ref, gain_ref,
                 gate_ref, up_ref, dn_ref, cos_row, cos_col, sin_row, sin_col,
                 out_ref,
                 q_ref, kv_ref, kvs, vt, top_s, sum_s, acc_s, proj, from_core, outgo, from_x,
                 squares, block, mid_ref, normed_ref, gu_ref, gu_all, dn_all, gu_acc, hidden,
                 ratio, column, terms, d_core, d_out, d_y, d_x, relay, last_x, last_y,
                 s_z, r_z, s_f, s_y, r_y, s_c, r_c, s1, r1, s2, r2, s3, r3,
                 s_ax, r_ax, s_az, r_az, s_ar, r_ar, s_ac, r_ac,
                 s_rz, r_rz, s_gz, r_gz, s_gy, r_gy, s_dz, r_dz, s_dy, r_dy,
                 e1, f1, e2, f2, e3, f3, e4, f4, e5, f5):
    sp, tp, z, y, x, c = place()
    rows, own = res_ref.shape
    n_tp = 2 * nx
    half = rows // 2
    tile = 256 if rows % 256 == 0 else rows
    tiles = rows // tile
    depth, twice = gate_ref.shape
    units = twice // 2
    wide = dn_ref.shape[2]
    other = x * 2 + 1 - c
    u = lax.rem(z, 2)
    z_other = z + 1 - 2 * u
    nh = nz // 2
    inner = lax.rem(z // 2 + u, 2)
    flip = lax.rem(u + inner, 2)
    z_to, z_from, slots_z = [z_other], [z_other], [0]
    for d in range(1, nh):
        ahead = lax.rem(z // 2 + d, nh) * 2
        behind = lax.rem(z // 2 - d + nh, nh) * 2
        z_to += [ahead + flip, ahead + 1 - flip]
        z_from += [behind + flip, behind + 1 - flip]
        slots_z += [2 * d - 1 + inner, 2 * d - inner]
    xs = [lax.rem(x + j, nx) for j in range(nx)]
    back = [lax.rem(x - j + nx, nx) for j in range(nx)]
    y_peer = (z * 2 + 1 - y, tp)
    core_peer = (sp, other)
    z_pair = (z_other * 2 + y, tp)
    z_peers = [(k * 2 + y, tp) for k in z_to]
    far = range(nz - 1)
    row_peers = [(sp, xs[j] * 2 + c) for j in range(1, nx)]
    across = [(sp, xs[j] * 2 + 1 - c) for j in range(1, nx)]

    def turn(ref, gain, columns, i):
        at = rows_at(i, GRID)
        v = ref[at, columns].astype(F32)
        v = v * lax.rsqrt(jnp.mean(v * v, axis=1, keepdims=True) + eps) * gain[...]
        row = sp * (rows // GRID) + i
        cosine = cos_row[pl.ds(row, 1), :] + cos_col[...]
        sine = sin_row[pl.ds(row, 1), :] + sin_col[...]
        return at, (v * cosine + pltpu.roll(v, HEAD_SIZE // 2, 1) * sine).astype(BF16)

    barrier = pltpu.get_barrier_semaphore()
    friends = z_peers + [y_peer, core_peer] + row_peers + across
    for to_sp, to_tp in friends:
        pl.semaphore_signal(
            barrier, inc=1, device_id={"sp": to_sp, "tp": to_tp}, device_id_type=MESH
        )

    with jax.named_scope("prep"):
        shared = pl.ds(
            pl.multiple_of(tp * heads // (QUERY_HEADS // KEY_VALUE_HEADS) * HEAD_SIZE, HEAD_SIZE),
            HEAD_SIZE,
        )

        @pl.loop(0, rows // GRID, unroll=4)
        def _(i):
            at, turned = turn(k_in, k_gain, shared, i)
            kv_ref[at, 0:HEAD_SIZE] = turned
            kv_ref[at, HEAD_SIZE:] = v_in[at, shared]

        for part in range(2):
            cut = slice(part * units, (part + 1) * units)
            for i in range(0, depth, 64):
                gu_ref[part, i : i + 64, :] = jnp.concatenate(
                    [gate_ref[i : i + 64, cut].astype(F32), up_ref[i : i + 64, cut].astype(F32)],
                    axis=1,
                ).astype(BF16)

    with jax.named_scope("greet"):
        pl.semaphore_wait(barrier, len(friends))

    def spot(owner, side):
        return kvs.at[pl.ds(pl.multiple_of(owner * rows + side * half, half), half), :]

    sends = []

    def describe(src, dst, out, arrive, slot, to):
        copy = pltpu.make_async_remote_copy(
            src_ref=src, dst_ref=dst, send_sem=out.at[slot], recv_sem=arrive.at[slot],
            device_id={"sp": to[0], "tp": to[1]}, device_id_type=MESH,
        )
        sends.append(copy)
        return copy

    def send(src, dst, out, arrive, slot, to):
        copy = remote(src, dst, out.at[slot], arrive.at[slot], *to)
        sends.append(copy)
        return copy

    def got(name, copy):
        with jax.named_scope("w_" + name):
            copy.wait_recv()

    mine = kv_ref.at[rows_at(c, half), :]
    send(mine, spot(sp, c), s_z, r_z, 0, z_pair)
    key_from = [(z_other, 0)]
    for d in range(1, nh):
        ahead = lax.rem(z // 2 + d, nh)
        behind = lax.rem(z // 2 - d + nh, nh)
        target = ((ahead * 2 + lax.rem(ahead + 1, 2)) * 2 + y, tp)
        send(mine, spot(sp, c), s_z, r_z, 2 * d - 1 + u, target)
        key_from += [(behind * 2 + uu, 2 * d - 1 + uu) for uu in range(2)]
    passed = []
    ky = [send(mine, spot(sp, c), s_y, r_y, 0, y_peer)]
    gz, gy, dz, dy = {}, {}, {}, {}

    def pieces(k):
        return 1 if k <= 0 else 2

    def gu_at(owner, k, a):
        size = depth // pieces(k)
        return gu_all.at[pl.ds(pl.multiple_of(owner * depth + a * size, size), size), :]

    def give_gu(k):
        for a in range(pieces(k)):
            size = depth // pieces(k)
            gz[k, a] = describe(gu_ref.at[lax.rem(z_to[k], 2), pl.ds(a * size, size)],
                                gu_at(sp, k, a), s_gz, r_gz, slots_z[k] * 2 + a, z_peers[k])

    def dn_at(owner, k, a):
        size = units // pieces(k)
        return dn_all.at[pl.ds(a * size, size), rows_at(owner, wide)]

    def give_dn(k):
        for a in range(pieces(k)):
            size = units // pieces(k)
            dz[k, a] = describe(dn_ref.at[lax.rem(z_to[k], 2), pl.ds(a * size, size)],
                                dn_at(sp, k, a), s_dz, r_dz, slots_z[k] * 2 + a, z_peers[k])

    dy[-1, 0] = send(dn_ref.at[u], dn_all.at[:, rows_at(sp, wide)], s_dy, r_dy, 0, y_peer)
    for k in far:
        give_gu(k)
        give_dn(k)

    def give_pair():
        gz[0, 0].start()

    pl.when(inner == 0)(give_pair)
    dz[0, 0].start()
    for k in far[1:]:
        for a in range(pieces(k)):
            gz[k, a].start()
    kvs[rows_at(sp, rows), :] = kv_ref[...]
    gu_all[rows_at(sp, depth), :] = gu_ref[u]
    dn_all[:, rows_at(sp, wide)] = dn_ref[u]

    with jax.named_scope("prep_q"):
        for h in range(heads):
            columns = slice(h * HEAD_SIZE, (h + 1) * HEAD_SIZE)

            @pl.loop(0, rows // GRID, unroll=4)
            def _(i):
                at, turned = turn(q_in, q_gain, columns, i)
                q_ref[at, columns] = turned

        top_s[...] = jnp.full(top_s.shape, -1e30, F32)
        sum_s[...] = jnp.zeros(sum_s.shape, F32)
        acc_s[...] = jnp.zeros(acc_s.shape, F32)
    factor = HEAD_SIZE ** (-0.5) * 1.4426950408889634

    def turn_values(owner):
        vt[owner] = kvs[rows_at(owner, rows), HEAD_SIZE:].astype(F32).T.astype(BF16)

    def attend(owner, start, stop):
        at = rows_at(owner, rows)
        with jax.named_scope("attend"):

            @pl.loop(start, stop)
            def _(i):
                slots = [i * heads + h for h in range(heads)]
                states = [(top_s[n], sum_s[n], acc_s[n]) for n in slots]
                scores = [
                    lax.dot_general(
                        kvs[at, 0:HEAD_SIZE],
                        q_ref[rows_at(i, tile), h * HEAD_SIZE : (h + 1) * HEAD_SIZE],
                        (((1,), (1,)), ((), ())), preferred_element_type=F32,
                    )
                    for h in range(heads)
                ]
                values = vt[owner]
                for n, s, (top, total, acc) in zip(slots, scores, states):
                    new_top = jnp.maximum(top, jnp.max(s, axis=0, keepdims=True))
                    fade = jnp.exp2((top - new_top) * factor)
                    w = jnp.exp2((s - new_top) * factor)
                    top_s[n] = new_top
                    sum_s[n] = total * fade + jnp.sum(w, axis=0, keepdims=True)
                    acc_s[n] = acc * fade + jnp.dot(
                        values, w.astype(BF16), preferred_element_type=F32
                    )

    kc = {}
    first = max(tiles - 1, 1)

    def to_core(at, slot):
        kc[slot] = send(at, at, s_c, r_c, slot, core_peer)

    def near_arrived(k):
        plane, slot = key_from[k]
        at = spot(plane * 2 + y, c)
        copy = pltpu.make_async_remote_copy(
            src_ref=at, dst_ref=at, send_sem=s_f.at[slot], recv_sem=r_z.at[slot],
            device_id={"sp": z_pair[0], "tp": tp}, device_id_type=MESH,
        )
        got("kz", copy)
        if k > 0:
            passed.append(copy)

            @pl.when(inner == 1)
            def _():
                copy.start()

        ky.append(send(at, at, s_y, r_y, k + 1, y_peer))
        to_core(at, 2 * k + 1)

    def far_arrived(k):
        got("ky", ky[k])
        to_core(spot((z if k == 0 else key_from[k - 1][0]) * 2 + 1 - y, c), 2 * k)

    def use(slot, owner):
        got("kc", kc[slot])
        turn_values(owner)
        attend(owner, 0, first)

    turn_values(sp)
    attend(sp, 0, first)
    far_arrived(0)
    near_arrived(0)
    use(0, z * 2 + 1 - y)
    for k in far:
        if k + 1 in far:
            near_arrived(k + 1)
        else:
            far_arrived(1)
        if k == far[-2]:
            pl.when(inner == 1)(give_pair)
            gy[-1, 0] = send(gu_ref.at[u], gu_all.at[rows_at(sp, depth), :], s_gy, r_gy, 0, y_peer)
        use(2 * k + 1, key_from[k][0] * 2 + y)
    for k in far:
        if k + 1 in far:
            far_arrived(k + 2)
        use(2 * k + 2, key_from[k][0] * 2 + 1 - y)

    def cols(t):
        return rows_at(t, own)

    def project(i):
        with jax.named_scope("proj"):
            parts = [
                (acc_s[i * heads + h] / sum_s[i * heads + h]).astype(BF16) for h in range(heads)
            ]
            whole = jnp.concatenate(parts, axis=0) if heads > 1 else parts[0]
            proj[rows_at(i, tile), :] = lax.dot_general(
                whole, w_ref[...], (((0,), (0,)), ((), ())), preferred_element_type=F32
            ).astype(BF16)

    near, to_x = {}, {}
    step = rows // 8
    small = tile // 4

    def give_core(t):
        at = pl.ds(t * tile, tile)
        for j in list(range(1, nx)) + [0]:
            near[t, j] = send(proj.at[at, cols(xs[j] * 2 + 1 - c)], from_core.at[j, at],
                              s1, r1, t * nx + j, core_peer)

    def give_x(t):
        for j in range(1, nx):
            got("near", near[t, j])

            @pl.loop(0, 4)
            def _(i):
                at = pl.ds(pl.multiple_of(t * tile + i * small, small), small)
                outgo[j - 1, at, :] = (
                    proj[at, cols(xs[j] * 2 + c)].astype(F32) + from_core[j, at, :].astype(F32)
                ).astype(BF16)

            at = pl.ds(t * tile, tile)
            to_x[t, j] = send(outgo.at[j - 1, at], from_x.at[j - 1, at], s2, r2,
                              t * (nx - 1) + j - 1, row_peers[j - 1])
        got("near", near[t, 0])

    def later(begin, end):
        @pl.loop(begin, end)
        def _(b):
            attend(b, first, tiles)

    def relay_gu(k, a, condition=None):
        at = gu_at(z_from[k] * 2 + y, k, a)
        if (k, a) not in gy:
            slot = (k + 1) * 2 + a
            gy[k, a] = pltpu.make_async_remote_copy(
                src_ref=at, dst_ref=at, send_sem=s_gy.at[slot], recv_sem=r_gy.at[slot],
                device_id={"sp": y_peer[0], "tp": y_peer[1]}, device_id_type=MESH,
            )
            sends.append(gy[k, a])

        def pass_on():
            got("gz" + str(k) + str(a), gz[k, a])
            gy[k, a].start()

        if condition is None:
            pass_on()
        else:
            pl.when(condition)(pass_on)

    def have_gu(k):
        for a in range(pieces(k)):
            got("gy" + str(k), gy[k, a])

    def relay_dn(k, condition=None):
        for a in range(pieces(k)):
            at = dn_at(z_from[k] * 2 + y, k, a)
            if (k, a) not in dy:
                dy[k, a] = describe(at, at, s_dy, r_dy, (k + 1) * 2 + a, y_peer)

        def pass_on():
            for a in range(pieces(k)):
                got("dz" + str(k), dz[k, a])
                dy[k, a].start()

        if condition is None:
            pass_on()
        else:
            pl.when(condition)(pass_on)

    for t in range(first):
        project(t)
        give_core(t)
    relay_gu(0, 0, inner == 1)
    relay_dn(0, inner == 0)
    if tiles > first:
        later(0, 2)
    for t in range(first):
        give_x(t)
    for t in range(first, tiles):
        later(2, 2 * nz)
        project(t)
        give_core(t)
    relay_dn(0, inner == 1)
    relay_gu(0, 0, inner == 0)
    for t in range(first, tiles):
        give_x(t)

    ones = jnp.ones((8, own), F32)
    peers = [core_peer] + row_peers + across
    az, ax, ac, ar = [], {}, {}, {}

    def home(uu, tt, t):
        return normed_ref.at[rows_at(uu * tiles + t, tile), cols(tt)]

    def on_core(uu, tt, t, slot):
        at = home(uu, tt, t)
        ac[t, slot] = send(at, at, s_ac, r_ac, t * 2 * nx + slot, core_peer)

    def add_up(t):
        for j in range(1, nx):
            got("tox", to_x[t, j])
        at = pl.ds(t * tile, tile)
        with jax.named_scope("mid"):
            total = proj[at, cols(tp)].astype(F32) + from_core[0, at, :].astype(F32)
            for j in range(1, nx):
                total += from_x[j - 1, at, :].astype(F32)
            mid = res_ref[at, :].astype(F32) + total
            mid_ref[at, :] = mid
            made = (mid * gain_ref[:, cols(tp)]).astype(BF16)
            block[at, :] = made
            normed_ref[rows_at(u * tiles + t, tile), cols(tp)] = made
            squares[0, :, at] = lax.dot_general(
                ones, mid * mid, (((1,), (1,)), ((), ())),
                precision=lax.Precision.HIGHEST, preferred_element_type=F32,
            )
        az.append(send(block.at[at], home(u, tp, t), s_az, r_az, t, z_pair))
        for j in range(1, nx):
            ax[t, j] = send(block.at[at], home(u, tp, t), s_ax, r_ax, t * (nx - 1) + j - 1,
                            row_peers[j - 1])
        ac[t, 0] = send(block.at[at], home(u, tp, t), s_ac, r_ac, t * 2 * nx, core_peer)

    for t in range(tiles):
        add_up(t)
        if t == 0:
            for k in far[1:2]:
                relay_gu(k, 0, inner == 1)
    sq = [send(squares.at[0], squares.at[k + 1], s3, r3, k, peers[k]) for k in range(len(peers))]
    for k in far[1:]:
        for a in range(2):
            dz[k, a].start()
    def gate_up(plane, uu, fresh=False):
        ks = rows_at(plane, 2 * depth)
        with jax.named_scope("gate_up"):
            @pl.loop(0, rows // 384)
            def _(i):
                at = pl.ds(pl.multiple_of(uu * rows + i * 384, 384), 384)
                term = jnp.dot(normed_ref[at, ks], gu_all[ks, :], preferred_element_type=F32)
                gu_acc[at, :] = term if fresh else gu_acc[at, :] + term

    for k in far[1:2]:
        relay_gu(k, 0, inner == 0)
    for t in range(tiles):
        for j in range(1, nx):
            got("ax", ax[t, j])
            on_core(u, back[j] * 2 + c, t, j)
    for t in range(tiles):
        for j in range(nx):
            got("ac", ac[t, j])
    have_gu(-1)
    gate_up(z, u, True)
    for k in far[1:2]:
        relay_gu(k, 1)
    have_gu(0)
    gate_up(z_from[0], u)
    for k in far[2:3]:
        relay_gu(k, 0)
    for t in range(tiles):
        if t == tiles - 1:
            for k in far[2:3]:
                relay_gu(k, 1)
        got("az", az[t])
        there = home(1 - u, tp, t)
        for j in range(1, nx):
            ar[t, j] = send(there, there, s_ar, r_ar, t * (nx - 1) + j - 1, row_peers[j - 1])
        on_core(1 - u, tp, t, nx)
    for copy in sq:
        got("sq", copy)
    with jax.named_scope("norm"):
        square = squares[0]
        for k in range(len(peers)):
            square += squares[k + 1]
        ratio[u] = lax.rsqrt(square / (n_tp * own) + eps)
    ratio_z = send(ratio.at[u], ratio.at[u], s_rz, r_rz, 0, z_pair)
    for k in far[3:]:
        for a in range(2):
            relay_gu(k, a)
    for t in range(tiles):
        for j in range(1, nx):
            got("ar", ar[t, j])
            on_core(1 - u, back[j] * 2 + c, t, nx + j)
    for k in far[1:2]:
        relay_dn(k, inner == 1)
    for t in range(tiles):
        for j in range(nx, 2 * nx):
            got("ac", ac[t, j])
    gate_up(z, 1 - u, True)
    gate_up(z_from[0], 1 - u)
    for k in far[2:3]:
        relay_dn(k, inner == 1)
    for k in far[3:]:
        relay_dn(k)
    for k in far[1:]:
        if k == 2:
            relay_dn(1, inner == 0)
            relay_dn(2, inner == 0)
        have_gu(k)
        gate_up(z_from[k], 1 - u)
        gate_up(z_from[k], u)

    got("ratio", ratio_z)
    for uu in range(2):
        column[pl.ds(uu * rows, rows), :] = ratio[uu].T
    with jax.named_scope("hidden"):
        for uu in range(2):
            @pl.loop(0, rows // 128)
            def _(i):
                at = pl.ds(pl.multiple_of(uu * rows + i * 128, 128), 128)
                scale = column[at, 0:1]
                gate = gu_acc[at, :units] * scale
                hidden[at, :] = (
                    gate / (1.0 + jnp.exp(-gate)) * (gu_acc[at, units:] * scale)
                ).astype(BF16)

    top, low = pl.ds(0, half), pl.ds(half, half)
    x_peers = [(sp, xs[j] * 2 + c) for j in range(nx)]
    every = [(1 - u, xs[j]) for j in range(nx)] + [(u, xs[j]) for j in range(1, nx)] + [(u, x)]
    turns = list(range(1, 2 * nx - 1)) + [0, 2 * nx - 1]
    side, to_z, to_x, again = {}, {}, {}, []
    which = [y, 1 - y]

    def sub(v):
        return rows_at(which[v], wide)

    def block_at(t, v):
        return rows_at(t * 2 + which[v], wide)

    def down(k, v):
        uu, xx = every[k]
        at = rows_at(uu, rows)
        with jax.named_scope("down"):
            for core in range(2):
                ks = block_at(xx * 2 + core, v)
                terms[at, ks] = jnp.dot(
                    hidden[at, :], dn_all[:, ks], preferred_element_type=F32
                ).astype(BF16)
        side[k, v] = send(terms.at[at, block_at(xx * 2 + 1 - c, v)], d_core.at[k, :, sub(v)],
                          e1, f1, 2 * k + v, core_peer)

    def forward(k, v):
        uu, xx = every[k]
        got("side", side[k, v])

        @pl.loop(0, 4)
        def _(i):
            at = rows_at(i, 2 * step)
            here = pl.ds(pl.multiple_of(uu * rows + i * 2 * step, 2 * step), 2 * step)
            d_out[k, at, sub(v)] = (
                terms[here, block_at(xx * 2 + c, v)].astype(F32)
                + d_core[k, at, sub(v)].astype(F32)
            ).astype(BF16)

        if k < nx:
            to_z[k, v] = send(d_out.at[k, top, sub(v)], d_y.at[k, :, sub(v)],
                              e2, f2, 2 * k + v, z_pair)
        j = k if k < nx else k - nx + 1
        if j > 0:
            slot = 2 * (j - 1) + (1 if k < nx else 0)
            to_x[slot, v] = send(d_out.at[k, low, sub(v)], d_x.at[slot, :, sub(v)],
                                 e3, f3, 2 * slot + v, x_peers[j])

    for v in range(2):
        if v == 1:
            for k in [-1] + list(far):
                for a in range(pieces(k)):
                    got("dy", dy[k, a])
        for i, k in enumerate(turns):
            down(k, v)
            if i > 0:
                forward(turns[i - 1], v)

    for v in range(2):
        for j in range(1, nx):
            got("to_z", to_z[j, v])

            @pl.loop(0, 4)
            def _(i):
                at = rows_at(i, step)
                relay[j, at, sub(v)] = (
                    d_out[nx + j - 1, at, sub(v)].astype(F32) + d_y[j, at, sub(v)].astype(F32)
                ).astype(BF16)

            again.append(send(relay.at[j, :, sub(v)], last_x.at[j - 1, :, sub(v)],
                              e4, f4, 2 * (j - 1) + v, x_peers[j]))
        for j in range(1, nx):
            got("to_x", to_x[2 * j - 1, v])

        @pl.loop(0, 4)
        def _(i):
            at = rows_at(i, step)
            here = pl.ds(pl.multiple_of(half + i * step, step), step)
            total = d_out[0, here, sub(v)].astype(F32)
            for j in range(1, nx):
                total += d_x[2 * j - 1, at, sub(v)].astype(F32)
            relay[0, at, sub(v)] = total.astype(BF16)

        again.append(send(relay.at[0, :, sub(v)], last_y.at[:, sub(v)], e5, f5, v, z_pair))
    for v in range(2):
        got("side", side[2 * nx - 1, v])
        got("to_z", to_z[0, v])
        for j in range(1, nx):
            got("to_x", to_x[2 * j - 2, v])
    for copy in again:
        got("again", copy)

    with jax.named_scope("final"):
        @pl.loop(0, 4)
        def _(i):
            at = rows_at(i, step)
            for part in range(2):
                to = pl.ds(pl.multiple_of(part * half + i * step, step), step)
                here = pl.ds(pl.multiple_of(u * rows + part * half + i * step, step), step)
                total = terms[here, cols(tp)].astype(F32)
                total += d_core[2 * nx - 1, to, :].astype(F32)
                total += (d_y[0, at, :] if part == 0 else last_y[at, :]).astype(F32)
                for j in range(1, nx):
                    total += (last_x[j - 1, at, :] if part == 0
                              else d_x[2 * j - 2, at, :]).astype(F32)
                out_ref[to, :] = (mid_ref[to, :] + 0.5 * total).astype(BF16)

    with jax.named_scope("w_sends"):
        @pl.when(inner == 1)
        def _():
            for copy in passed:
                copy.wait_send()

        for copy in sends:
            copy.wait_send()


def layer(q, k, v, q_gain, k_gain, w, res, gain, gate, up, dn, n_sp, n_tp):
    nz, nx = n_sp // 2, n_tp // 2
    rows, own = res.shape
    heads = q.shape[1] // HEAD_SIZE
    tile = 256 if rows % 256 == 0 else rows
    tiles = rows // tile
    count = heads * tiles
    width = n_tp * own
    depth, twice = gate.shape
    wide = dn.shape[2]
    dma = pltpu.SemaphoreType.DMA
    n = 2 * nx
    vm = pl.BlockSpec(memory_space=pltpu.VMEM)

    def two(k):
        return [dma((k,)), dma((k,))]

    def bf(*shape):
        return pltpu.VMEM(shape, BF16)

    def fl(*shape):
        return pltpu.VMEM(shape, F32)

    return pl.pallas_call(
        functools.partial(layer_kernel, nz, nx, heads),
        out_shape=jax.ShapeDtypeStruct((rows, own), BF16),
        in_specs=[vm] * 15,
        out_specs=vm,
        scratch_shapes=[
            bf(rows, heads * HEAD_SIZE), bf(rows, 2 * HEAD_SIZE),
            bf(n_sp * rows, 2 * HEAD_SIZE), bf(n_sp, HEAD_SIZE, rows),
            fl(count, 1, tile), fl(count, 1, tile), fl(count, HEAD_SIZE, tile),
            bf(rows, width), bf(nx, rows, own), bf(nx - 1, rows, own), bf(nx - 1, rows, own),
            fl(n, 8, rows), bf(rows, own), fl(rows, own), bf(2 * rows, width),
            bf(2, depth, twice), bf(n_sp * depth, twice), bf(dn.shape[1], n_sp * wide),
            fl(2 * rows, twice), bf(2 * rows, twice // 2), fl(2, 8, rows), fl(2 * rows, 8), bf(2 * rows, width),
            bf(n, rows, own), bf(n - 1, rows, own), bf(nx, rows // 2, own),
            bf(n - 2, rows // 2, own), bf(nx, rows // 2, own), bf(nx - 1, rows // 2, own),
            bf(rows // 2, own),
        ] + two(nz - 1) + [dma((nz - 1,))] + two(nz) + two(2 * nz - 1)
        + two(tiles * nx) + two(tiles * (nx - 1)) + two(n - 1)
        + two(tiles * (nx - 1)) + two(tiles) + two(tiles * (nx - 1)) + two(tiles * 2 * nx)
        + two(1) + two(2 * nz) + two(2 * nz) + two(2 * nz) + two(2 * nz)
        + two(2 * n) + two(2 * nx) + two(2 * n - 4) + two(2 * nx - 2) + two(2),
        compiler_params=pltpu.CompilerParams(
            collective_id=0, has_side_effects=True, vmem_limit_bytes=VMEM_LIMIT
        ),
        name="layer",
    )(q, k, v, q_gain, k_gain, w, res, gain, gate, up, dn, *rotary_tables(n_sp * rows))


def on_device(n_sp, n_tp, residual_in, queries, keys, values, query_gain, key_norm_gain,
              out_weight, mlp_gain, gate_weight, up_weight, down_weight):
    down = down_weight.reshape(2, down_weight.shape[0] // 2, down_weight.shape[1])
    return layer(
        queries, keys, values, query_gain[None, :], key_norm_gain[None, :], out_weight,
        residual_in, mlp_gain[None, :], gate_weight, up_weight, down, n_sp, n_tp,
    )


def solution(mesh):
    in_specs = (
        P("sp", "tp"),
        P("sp", "tp"),
        P("sp", None),
        P("sp", None),
        P(),
        P(),
        P("tp", None),
        P(),
        P("sp", "tp"),
        P("sp", "tp"),
        P("tp", "sp"),
    )
    out_specs = P("sp", "tp")
    return jax.shard_map(
        functools.partial(on_device, mesh.shape["sp"], mesh.shape["tp"]),
        mesh=mesh, in_specs=in_specs, out_specs=out_specs, check_vma=False,
    )
```

```python
import functools
import jax
import numpy as np
import jax.numpy as jnp
from jax import lax
from jax.experimental import pallas as pl
from jax.experimental.pallas import tpu as pltpu
from jax.sharding import PartitionSpec as P

D = 2048
HEAD_SIZE = 128
QUERY_HEADS = 8
KEY_VALUE_HEADS = 2
GRID = 64

eps = 1e-06
rotary_base = 10000.0
MESH = pl.DeviceIdType.MESH
VMEM_LIMIT = 67043328
F32 = jnp.float32
BF16 = jnp.bfloat16


def remote(src, dst, send, recv, sp, tp):
    copy = pltpu.make_async_remote_copy(
        src_ref=src, dst_ref=dst, send_sem=send, recv_sem=recv,
        device_id={"sp": sp, "tp": tp}, device_id_type=MESH,
    )
    copy.start()
    return copy


def greet(peers):
    barrier = pltpu.get_barrier_semaphore()
    for sp, tp in peers:
        pl.semaphore_signal(
            barrier, inc=1, device_id={"sp": sp, "tp": tp}, device_id_type=MESH
        )
    pl.semaphore_wait(barrier, len(peers))


def place():
    sp = lax.axis_index("sp")
    tp = lax.axis_index("tp")
    return sp, tp, sp // 2, lax.rem(sp, 2), tp // 2, lax.rem(tp, 2)


def rows_at(index, size):
    return pl.ds(pl.multiple_of(index * size, size), size)


def rotary_tables(tokens):
    half_size = HEAD_SIZE // 2
    frequency = np.float32(rotary_base) ** (
        -np.arange(0, half_size, 2, dtype=np.float32) / np.float32(half_size)
    )
    longest = max(tokens // GRID, GRID)
    angles = np.arange(longest, dtype=np.float32)[:, None] * frequency.astype(np.float32)
    cosine, sine = np.cos(angles), np.sin(angles)
    none = np.zeros_like(angles)
    rows = tokens // GRID
    pieces = [
        np.concatenate([cosine, none, cosine, none], axis=1)[:rows],
        np.concatenate([none, cosine, none, cosine], axis=1)[:GRID],
        np.concatenate([-sine, none, sine, none], axis=1)[:rows],
        np.concatenate([none, -sine, none, sine], axis=1)[:GRID],
    ]
    return [jnp.asarray(piece, F32) for piece in pieces]


def layer_kernel(nz, nx, heads, q_in, k_in, v_in, q_gain, k_gain, w_ref, res_ref, gain_ref,
                 gate_ref, up_ref, dn_ref, cos_row, cos_col, sin_row, sin_col,
                 out_ref,
                 q_ref, kv_ref, kvs, vt, top_s, sum_s, acc_s, proj, from_core, outgo, from_x,
                 squares, block, mid_ref, normed_ref, gu_ref, gu_all, dn_all, gu_acc, hidden,
                 ratio, column, terms, d_core, d_out, d_y, d_x, relay, last_x, last_y,
                 s_z, r_z, s_f, s_y, r_y, s_c, r_c, s1, r1, s2, r2, s3, r3,
                 s_ax, r_ax, s_az, r_az, s_ar, r_ar, s_ac, r_ac,
                 s_rz, r_rz, s_gz, r_gz, s_gy, r_gy, s_dz, r_dz, s_dy, r_dy,
                 e1, f1, e2, f2, e3, f3, e4, f4, e5, f5):
    sp, tp, z, y, x, c = place()
    rows, own = res_ref.shape
    n_tp = 2 * nx
    half = rows // 2
    tile = 256 if rows % 256 == 0 else rows
    tiles = rows // tile
    depth, twice = gate_ref.shape
    units = twice // 2
    wide = dn_ref.shape[2]
    other = x * 2 + 1 - c
    u = lax.rem(z, 2)
    z_other = z + 1 - 2 * u
    nh = nz // 2
    inner = lax.rem(z // 2 + u, 2)
    flip = lax.rem(u + inner, 2)
    z_to, z_from, slots_z = [z_other], [z_other], [0]
    for d in range(1, nh):
        ahead = lax.rem(z // 2 + d, nh) * 2
        behind = lax.rem(z // 2 - d + nh, nh) * 2
        z_to += [ahead + flip, ahead + 1 - flip]
        z_from += [behind + flip, behind + 1 - flip]
        slots_z += [2 * d - 1 + inner, 2 * d - inner]
    xs = [lax.rem(x + j, nx) for j in range(nx)]
    back = [lax.rem(x - j + nx, nx) for j in range(nx)]
    y_peer = (z * 2 + 1 - y, tp)
    core_peer = (sp, other)
    z_pair = (z_other * 2 + y, tp)
    z_peers = [(k * 2 + y, tp) for k in z_to]
    far = range(nz - 1)
    row_peers = [(sp, xs[j] * 2 + c) for j in range(1, nx)]
    across = [(sp, xs[j] * 2 + 1 - c) for j in range(1, nx)]

    def turn(ref, gain, columns, i):
        at = rows_at(i, GRID)
        v = ref[at, columns].astype(F32)
        v = v * lax.rsqrt(jnp.mean(v * v, axis=1, keepdims=True) + eps) * gain[...]
        row = sp * (rows // GRID) + i
        cosine = cos_row[pl.ds(row, 1), :] + cos_col[...]
        sine = sin_row[pl.ds(row, 1), :] + sin_col[...]
        return at, (v * cosine + pltpu.roll(v, HEAD_SIZE // 2, 1) * sine).astype(BF16)

    barrier = pltpu.get_barrier_semaphore()
    friends = z_peers + [y_peer, core_peer] + row_peers + across
    for to_sp, to_tp in friends:
        pl.semaphore_signal(
            barrier, inc=1, device_id={"sp": to_sp, "tp": to_tp}, device_id_type=MESH
        )

    with jax.named_scope("prep"):
        shared = pl.ds(
            pl.multiple_of(tp * heads // (QUERY_HEADS // KEY_VALUE_HEADS) * HEAD_SIZE, HEAD_SIZE),
            HEAD_SIZE,
        )

        @pl.loop(0, rows // GRID, unroll=4)
        def _(i):
            at, turned = turn(k_in, k_gain, shared, i)
            kv_ref[at, 0:HEAD_SIZE] = turned
            kv_ref[at, HEAD_SIZE:] = v_in[at, shared]

        for part in range(2):
            cut = slice(part * units, (part + 1) * units)
            for i in range(0, depth, 64):
                gu_ref[part, i : i + 64, :] = jnp.concatenate(
                    [gate_ref[i : i + 64, cut].astype(F32), up_ref[i : i + 64, cut].astype(F32)],
                    axis=1,
                ).astype(BF16)

    with jax.named_scope("greet"):
        pl.semaphore_wait(barrier, len(friends))

    def spot(owner, side):
        return kvs.at[pl.ds(pl.multiple_of(owner * rows + side * half, half), half), :]

    sends = []

    def describe(src, dst, out, arrive, slot, to):
        copy = pltpu.make_async_remote_copy(
            src_ref=src, dst_ref=dst, send_sem=out.at[slot], recv_sem=arrive.at[slot],
            device_id={"sp": to[0], "tp": to[1]}, device_id_type=MESH,
        )
        sends.append(copy)
        return copy

    def send(src, dst, out, arrive, slot, to):
        copy = remote(src, dst, out.at[slot], arrive.at[slot], *to)
        sends.append(copy)
        return copy

    def got(name, copy):
        with jax.named_scope("w_" + name):
            copy.wait_recv()

    mine = kv_ref.at[rows_at(c, half), :]
    send(mine, spot(sp, c), s_z, r_z, 0, z_pair)
    key_from = [(z_other, 0)]
    for d in range(1, nh):
        ahead = lax.rem(z // 2 + d, nh)
        behind = lax.rem(z // 2 - d + nh, nh)
        target = ((ahead * 2 + lax.rem(ahead + 1, 2)) * 2 + y, tp)
        send(mine, spot(sp, c), s_z, r_z, 2 * d - 1 + u, target)
        key_from += [(behind * 2 + uu, 2 * d - 1 + uu) for uu in range(2)]
    passed = []
    ky = [send(mine, spot(sp, c), s_y, r_y, 0, y_peer)]
    gz, gy, dz, dy = {}, {}, {}, {}

    def pieces(k):
        return 1 if k <= 0 else 2

    def gu_at(owner, k, a):
        size = depth // pieces(k)
        return gu_all.at[pl.ds(pl.multiple_of(owner * depth + a * size, size), size), :]

    def give_gu(k):
        for a in range(pieces(k)):
            size = depth // pieces(k)
            gz[k, a] = describe(gu_ref.at[lax.rem(z_to[k], 2), pl.ds(a * size, size)],
                                gu_at(sp, k, a), s_gz, r_gz, slots_z[k] * 2 + a, z_peers[k])

    def dn_at(owner, k, a):
        size = units // pieces(k)
        return dn_all.at[pl.ds(a * size, size), rows_at(owner, wide)]

    def give_dn(k):
        for a in range(pieces(k)):
            size = units // pieces(k)
            dz[k, a] = describe(dn_ref.at[lax.rem(z_to[k], 2), pl.ds(a * size, size)],
                                dn_at(sp, k, a), s_dz, r_dz, slots_z[k] * 2 + a, z_peers[k])

    dy[-1, 0] = send(dn_ref.at[u], dn_all.at[:, rows_at(sp, wide)], s_dy, r_dy, 0, y_peer)
    for k in far:
        give_gu(k)
        give_dn(k)

    def give_pair():
        gz[0, 0].start()

    pl.when(inner == 0)(give_pair)
    dz[0, 0].start()
    for k in far[1:]:
        for a in range(pieces(k)):
            gz[k, a].start()
    kvs[rows_at(sp, rows), :] = kv_ref[...]
    gu_all[rows_at(sp, depth), :] = gu_ref[u]
    dn_all[:, rows_at(sp, wide)] = dn_ref[u]

    with jax.named_scope("prep_q"):
        for h in range(heads):
            columns = slice(h * HEAD_SIZE, (h + 1) * HEAD_SIZE)

            @pl.loop(0, rows // GRID, unroll=4)
            def _(i):
                at, turned = turn(q_in, q_gain, columns, i)
                q_ref[at, columns] = turned

        top_s[...] = jnp.full(top_s.shape, -1e30, F32)
        sum_s[...] = jnp.zeros(sum_s.shape, F32)
        acc_s[...] = jnp.zeros(acc_s.shape, F32)
    factor = HEAD_SIZE ** (-0.5) * 1.4426950408889634

    def turn_values(owner):
        vt[owner] = kvs[rows_at(owner, rows), HEAD_SIZE:].astype(F32).T.astype(BF16)

    def attend(owner, start, stop):
        at = rows_at(owner, rows)
        with jax.named_scope("attend"):

            @pl.loop(start, stop)
            def _(i):
                slots = [i * heads + h for h in range(heads)]
                states = [(top_s[n], sum_s[n], acc_s[n]) for n in slots]
                scores = [
                    lax.dot_general(
                        kvs[at, 0:HEAD_SIZE],
                        q_ref[rows_at(i, tile), h * HEAD_SIZE : (h + 1) * HEAD_SIZE],
                        (((1,), (1,)), ((), ())), preferred_element_type=F32,
                    )
                    for h in range(heads)
                ]
                values = vt[owner]
                for n, s, (top, total, acc) in zip(slots, scores, states):
                    new_top = jnp.maximum(top, jnp.max(s, axis=0, keepdims=True))
                    fade = jnp.exp2((top - new_top) * factor)
                    w = jnp.exp2((s - new_top) * factor)
                    top_s[n] = new_top
                    sum_s[n] = total * fade + jnp.sum(w, axis=0, keepdims=True)
                    acc_s[n] = acc * fade + jnp.dot(
                        values, w.astype(BF16), preferred_element_type=F32
                    )

    kc = {}
    first = max(tiles - 1, 1)

    def to_core(at, slot):
        kc[slot] = send(at, at, s_c, r_c, slot, core_peer)

    def near_arrived(k):
        plane, slot = key_from[k]
        at = spot(plane * 2 + y, c)
        copy = pltpu.make_async_remote_copy(
            src_ref=at, dst_ref=at, send_sem=s_f.at[slot], recv_sem=r_z.at[slot],
            device_id={"sp": z_pair[0], "tp": tp}, device_id_type=MESH,
        )
        got("kz", copy)
        if k > 0:
            passed.append(copy)

            @pl.when(inner == 1)
            def _():
                copy.start()

        ky.append(send(at, at, s_y, r_y, k + 1, y_peer))
        to_core(at, 2 * k + 1)

    def far_arrived(k):
        got("ky", ky[k])
        to_core(spot((z if k == 0 else key_from[k - 1][0]) * 2 + 1 - y, c), 2 * k)

    def use(slot, owner):
        got("kc", kc[slot])
        turn_values(owner)
        attend(owner, 0, first)

    turn_values(sp)
    attend(sp, 0, first)
    far_arrived(0)
    near_arrived(0)
    use(0, z * 2 + 1 - y)
    for k in far:
        if k + 1 in far:
            near_arrived(k + 1)
        else:
            far_arrived(1)
        if k == far[-2]:
            pl.when(inner == 1)(give_pair)
            gy[-1, 0] = send(gu_ref.at[u], gu_all.at[rows_at(sp, depth), :], s_gy, r_gy, 0, y_peer)
        use(2 * k + 1, key_from[k][0] * 2 + y)
    for k in far:
        if k + 1 in far:
            far_arrived(k + 2)
        use(2 * k + 2, key_from[k][0] * 2 + 1 - y)

    def cols(t):
        return rows_at(t, own)

    def project(i):
        with jax.named_scope("proj"):
            parts = [
                (acc_s[i * heads + h] / sum_s[i * heads + h]).astype(BF16) for h in range(heads)
            ]
            whole = jnp.concatenate(parts, axis=0) if heads > 1 else parts[0]
            proj[rows_at(i, tile), :] = lax.dot_general(
                whole, w_ref[...], (((0,), (0,)), ((), ())), preferred_element_type=F32
            ).astype(BF16)

    near, to_x = {}, {}
    step = rows // 8
    small = tile // 4

    def give_core(t):
        at = pl.ds(t * tile, tile)
        for j in list(range(1, nx)) + [0]:
            near[t, j] = send(proj.at[at, cols(xs[j] * 2 + 1 - c)], from_core.at[j, at],
                              s1, r1, t * nx + j, core_peer)

    def give_x(t):
        for j in range(1, nx):
            got("near", near[t, j])

            @pl.loop(0, 4)
            def _(i):
                at = pl.ds(pl.multiple_of(t * tile + i * small, small), small)
                outgo[j - 1, at, :] = (
                    proj[at, cols(xs[j] * 2 + c)].astype(F32) + from_core[j, at, :].astype(F32)
                ).astype(BF16)

            at = pl.ds(t * tile, tile)
            to_x[t, j] = send(outgo.at[j - 1, at], from_x.at[j - 1, at], s2, r2,
                              t * (nx - 1) + j - 1, row_peers[j - 1])
        got("near", near[t, 0])

    def later(begin, end):
        @pl.loop(begin, end)
        def _(b):
            attend(b, first, tiles)

    def relay_gu(k, a, condition=None):
        at = gu_at(z_from[k] * 2 + y, k, a)
        if (k, a) not in gy:
            slot = (k + 1) * 2 + a
            gy[k, a] = pltpu.make_async_remote_copy(
                src_ref=at, dst_ref=at, send_sem=s_gy.at[slot], recv_sem=r_gy.at[slot],
                device_id={"sp": y_peer[0], "tp": y_peer[1]}, device_id_type=MESH,
            )
            sends.append(gy[k, a])

        def pass_on():
            got("gz" + str(k) + str(a), gz[k, a])
            gy[k, a].start()

        if condition is None:
            pass_on()
        else:
            pl.when(condition)(pass_on)

    def have_gu(k):
        for a in range(pieces(k)):
            got("gy" + str(k), gy[k, a])

    def relay_dn(k, condition=None):
        for a in range(pieces(k)):
            at = dn_at(z_from[k] * 2 + y, k, a)
            if (k, a) not in dy:
                dy[k, a] = describe(at, at, s_dy, r_dy, (k + 1) * 2 + a, y_peer)

        def pass_on():
            for a in range(pieces(k)):
                got("dz" + str(k), dz[k, a])
                dy[k, a].start()

        if condition is None:
            pass_on()
        else:
            pl.when(condition)(pass_on)

    for t in range(first):
        project(t)
        give_core(t)
    relay_gu(0, 0, inner == 1)
    relay_dn(0, inner == 0)
    if tiles > first:
        later(0, 2)
    for t in range(first):
        give_x(t)
    for t in range(first, tiles):
        later(2, 2 * nz)
        project(t)
        give_core(t)
    relay_dn(0, inner == 1)
    relay_gu(0, 0, inner == 0)
    for t in range(first, tiles):
        give_x(t)

    ones = jnp.ones((8, own), F32)
    peers = [core_peer] + row_peers + across
    az, ax, ac, ar = [], {}, {}, {}

    def home(uu, tt, t):
        return normed_ref.at[rows_at(uu * tiles + t, tile), cols(tt)]

    def on_core(uu, tt, t, slot):
        at = home(uu, tt, t)
        ac[t, slot] = send(at, at, s_ac, r_ac, t * 2 * nx + slot, core_peer)

    def add_up(t):
        for j in range(1, nx):
            got("tox", to_x[t, j])
        at = pl.ds(t * tile, tile)
        with jax.named_scope("mid"):
            total = proj[at, cols(tp)].astype(F32) + from_core[0, at, :].astype(F32)
            for j in range(1, nx):
                total += from_x[j - 1, at, :].astype(F32)
            mid = res_ref[at, :].astype(F32) + total
            mid_ref[at, :] = mid
            made = (mid * gain_ref[:, cols(tp)]).astype(BF16)
            block[at, :] = made
            normed_ref[rows_at(u * tiles + t, tile), cols(tp)] = made
            squares[0, :, at] = lax.dot_general(
                ones, mid * mid, (((1,), (1,)), ((), ())),
                precision=lax.Precision.HIGHEST, preferred_element_type=F32,
            )
        az.append(send(block.at[at], home(u, tp, t), s_az, r_az, t, z_pair))
        for j in range(1, nx):
            ax[t, j] = send(block.at[at], home(u, tp, t), s_ax, r_ax, t * (nx - 1) + j - 1,
                            row_peers[j - 1])
        ac[t, 0] = send(block.at[at], home(u, tp, t), s_ac, r_ac, t * 2 * nx, core_peer)

    for t in range(tiles):
        add_up(t)
        if t == 0:
            for k in far[1:2]:
                relay_gu(k, 0, inner == 1)
    sq = [send(squares.at[0], squares.at[k + 1], s3, r3, k, peers[k]) for k in range(len(peers))]
    for k in far[1:]:
        for a in range(2):
            dz[k, a].start()
    def gate_up(plane, uu, fresh=False):
        ks = rows_at(plane, 2 * depth)
        with jax.named_scope("gate_up"):
            @pl.loop(0, rows // 384)
            def _(i):
                at = pl.ds(pl.multiple_of(uu * rows + i * 384, 384), 384)
                term = jnp.dot(normed_ref[at, ks], gu_all[ks, :], preferred_element_type=F32)
                gu_acc[at, :] = term if fresh else gu_acc[at, :] + term

    for k in far[1:2]:
        relay_gu(k, 0, inner == 0)
    for t in range(tiles):
        for j in range(1, nx):
            got("ax", ax[t, j])
            on_core(u, back[j] * 2 + c, t, j)
    for t in range(tiles):
        for j in range(nx):
            got("ac", ac[t, j])
    have_gu(-1)
    gate_up(z, u, True)
    for k in far[1:2]:
        relay_gu(k, 1)
    have_gu(0)
    gate_up(z_from[0], u)
    for k in far[2:3]:
        relay_gu(k, 0)
    for t in range(tiles):
        if t == tiles - 1:
            for k in far[2:3]:
                relay_gu(k, 1)
        got("az", az[t])
        there = home(1 - u, tp, t)
        for j in range(1, nx):
            ar[t, j] = send(there, there, s_ar, r_ar, t * (nx - 1) + j - 1, row_peers[j - 1])
        on_core(1 - u, tp, t, nx)
    for copy in sq:
        got("sq", copy)
    with jax.named_scope("norm"):
        square = squares[0]
        for k in range(len(peers)):
            square += squares[k + 1]
        ratio[u] = lax.rsqrt(square / (n_tp * own) + eps)
    ratio_z = send(ratio.at[u], ratio.at[u], s_rz, r_rz, 0, z_pair)
    for k in far[3:]:
        for a in range(2):
            relay_gu(k, a)
    for t in range(tiles):
        for j in range(1, nx):
            got("ar", ar[t, j])
            on_core(1 - u, back[j] * 2 + c, t, nx + j)
    for k in far[1:2]:
        relay_dn(k, inner == 1)
    for t in range(tiles):
        for j in range(nx, 2 * nx):
            got("ac", ac[t, j])
    gate_up(z, 1 - u, True)
    gate_up(z_from[0], 1 - u)
    for k in far[2:3]:
        relay_dn(k, inner == 1)
    for k in far[3:]:
        relay_dn(k)
    for k in far[1:]:
        if k == 2:
            relay_dn(1, inner == 0)
            relay_dn(2, inner == 0)
        have_gu(k)
        gate_up(z_from[k], 1 - u)
        gate_up(z_from[k], u)

    got("ratio", ratio_z)
    for uu in range(2):
        column[pl.ds(uu * rows, rows), :] = ratio[uu].T
    def activate(uu):
        with jax.named_scope("hidden"):
            @pl.loop(0, rows // 128)
            def _(i):
                at = pl.ds(pl.multiple_of(uu * rows + i * 128, 128), 128)
                scale = column[at, 0:1]
                gate = gu_acc[at, :units] * scale
                hidden[at, :] = (
                    gate / (1.0 + jnp.exp(-gate)) * (gu_acc[at, units:] * scale)
                ).astype(BF16)

    activate(1 - u)
    top, low = pl.ds(0, half), pl.ds(half, half)
    x_peers = [(sp, xs[j] * 2 + c) for j in range(nx)]
    every = [(1 - u, xs[j]) for j in range(nx)] + [(u, xs[j]) for j in range(1, nx)] + [(u, x)]
    turns = list(range(1, 2 * nx - 1)) + [0, 2 * nx - 1]
    side, to_z, to_x, again = {}, {}, {}, []
    which = [y, 1 - y]

    def sub(v):
        return rows_at(which[v], wide)

    def block_at(t, v):
        return rows_at(t * 2 + which[v], wide)

    def down(k, v):
        uu, xx = every[k]
        at = rows_at(uu, rows)
        with jax.named_scope("down"):
            for core in range(2):
                ks = block_at(xx * 2 + core, v)
                terms[at, ks] = jnp.dot(
                    hidden[at, :], dn_all[:, ks], preferred_element_type=F32
                ).astype(BF16)
        side[k, v] = send(terms.at[at, block_at(xx * 2 + 1 - c, v)], d_core.at[k, :, sub(v)],
                          e1, f1, 2 * k + v, core_peer)

    def forward(k, v):
        uu, xx = every[k]
        got("side", side[k, v])

        @pl.loop(0, 4)
        def _(i):
            at = rows_at(i, 2 * step)
            here = pl.ds(pl.multiple_of(uu * rows + i * 2 * step, 2 * step), 2 * step)
            d_out[k, at, sub(v)] = (
                terms[here, block_at(xx * 2 + c, v)].astype(F32)
                + d_core[k, at, sub(v)].astype(F32)
            ).astype(BF16)

        if k < nx:
            to_z[k, v] = send(d_out.at[k, top, sub(v)], d_y.at[k, :, sub(v)],
                              e2, f2, 2 * k + v, z_pair)
        j = k if k < nx else k - nx + 1
        if j > 0:
            slot = 2 * (j - 1) + (1 if k < nx else 0)
            to_x[slot, v] = send(d_out.at[k, low, sub(v)], d_x.at[slot, :, sub(v)],
                                 e3, f3, 2 * slot + v, x_peers[j])

    for v in range(2):
        if v == 1:
            for k in [-1] + list(far):
                for a in range(pieces(k)):
                    got("dy", dy[k, a])
        for i, k in enumerate(turns):
            down(k, v)
            if i == 0 and v == 0:
                activate(u)
            if i > 0:
                forward(turns[i - 1], v)

        for j in range(1, nx):
            got("to_z", to_z[j, v])

            @pl.loop(0, 4)
            def _(i):
                at = rows_at(i, step)
                relay[j, at, sub(v)] = (
                    d_out[nx + j - 1, at, sub(v)].astype(F32) + d_y[j, at, sub(v)].astype(F32)
                ).astype(BF16)

            again.append(send(relay.at[j, :, sub(v)], last_x.at[j - 1, :, sub(v)],
                              e4, f4, 2 * (j - 1) + v, x_peers[j]))
        for j in range(1, nx):
            got("to_x", to_x[2 * j - 1, v])

        @pl.loop(0, 4)
        def _(i):
            at = rows_at(i, step)
            here = pl.ds(pl.multiple_of(half + i * step, step), step)
            total = d_out[0, here, sub(v)].astype(F32)
            for j in range(1, nx):
                total += d_x[2 * j - 1, at, sub(v)].astype(F32)
            relay[0, at, sub(v)] = total.astype(BF16)

        again.append(send(relay.at[0, :, sub(v)], last_y.at[:, sub(v)], e5, f5, v, z_pair))
    for v in range(2):
        got("side", side[2 * nx - 1, v])
        got("to_z", to_z[0, v])
        for j in range(1, nx):
            got("to_x", to_x[2 * j - 2, v])
    for copy in again:
        got("again", copy)

    with jax.named_scope("final"):
        @pl.loop(0, 4)
        def _(i):
            at = rows_at(i, step)
            for part in range(2):
                to = pl.ds(pl.multiple_of(part * half + i * step, step), step)
                here = pl.ds(pl.multiple_of(u * rows + part * half + i * step, step), step)
                total = terms[here, cols(tp)].astype(F32)
                total += d_core[2 * nx - 1, to, :].astype(F32)
                total += (d_y[0, at, :] if part == 0 else last_y[at, :]).astype(F32)
                for j in range(1, nx):
                    total += (last_x[j - 1, at, :] if part == 0
                              else d_x[2 * j - 2, at, :]).astype(F32)
                out_ref[to, :] = (mid_ref[to, :] + 0.5 * total).astype(BF16)

    with jax.named_scope("w_sends"):
        @pl.when(inner == 1)
        def _():
            for copy in passed:
                copy.wait_send()

        for copy in sends:
            copy.wait_send()


def layer(q, k, v, q_gain, k_gain, w, res, gain, gate, up, dn, n_sp, n_tp):
    nz, nx = n_sp // 2, n_tp // 2
    rows, own = res.shape
    heads = q.shape[1] // HEAD_SIZE
    tile = 256 if rows % 256 == 0 else rows
    tiles = rows // tile
    count = heads * tiles
    width = n_tp * own
    depth, twice = gate.shape
    wide = dn.shape[2]
    dma = pltpu.SemaphoreType.DMA
    n = 2 * nx
    vm = pl.BlockSpec(memory_space=pltpu.VMEM)

    def two(k):
        return [dma((k,)), dma((k,))]

    def bf(*shape):
        return pltpu.VMEM(shape, BF16)

    def fl(*shape):
        return pltpu.VMEM(shape, F32)

    return pl.pallas_call(
        functools.partial(layer_kernel, nz, nx, heads),
        out_shape=jax.ShapeDtypeStruct((rows, own), BF16),
        in_specs=[vm] * 15,
        out_specs=vm,
        scratch_shapes=[
            bf(rows, heads * HEAD_SIZE), bf(rows, 2 * HEAD_SIZE),
            bf(n_sp * rows, 2 * HEAD_SIZE), bf(n_sp, HEAD_SIZE, rows),
            fl(count, 1, tile), fl(count, 1, tile), fl(count, HEAD_SIZE, tile),
            bf(rows, width), bf(nx, rows, own), bf(nx - 1, rows, own), bf(nx - 1, rows, own),
            fl(n, 8, rows), bf(rows, own), fl(rows, own), bf(2 * rows, width),
            bf(2, depth, twice), bf(n_sp * depth, twice), bf(dn.shape[1], n_sp * wide),
            fl(2 * rows, twice), bf(2 * rows, twice // 2), fl(2, 8, rows), fl(2 * rows, 8), bf(2 * rows, width),
            bf(n, rows, own), bf(n - 1, rows, own), bf(nx, rows // 2, own),
            bf(n - 2, rows // 2, own), bf(nx, rows // 2, own), bf(nx - 1, rows // 2, own),
            bf(rows // 2, own),
        ] + two(nz - 1) + [dma((nz - 1,))] + two(nz) + two(2 * nz - 1)
        + two(tiles * nx) + two(tiles * (nx - 1)) + two(n - 1)
        + two(tiles * (nx - 1)) + two(tiles) + two(tiles * (nx - 1)) + two(tiles * 2 * nx)
        + two(1) + two(2 * nz) + two(2 * nz) + two(2 * nz) + two(2 * nz)
        + two(2 * n) + two(2 * nx) + two(2 * n - 4) + two(2 * nx - 2) + two(2),
        compiler_params=pltpu.CompilerParams(
            collective_id=0, has_side_effects=True, vmem_limit_bytes=VMEM_LIMIT
        ),
        name="layer",
    )(q, k, v, q_gain, k_gain, w, res, gain, gate, up, dn, *rotary_tables(n_sp * rows))


def on_device(n_sp, n_tp, residual_in, queries, keys, values, query_gain, key_norm_gain,
              out_weight, mlp_gain, gate_weight, up_weight, down_weight):
    down = down_weight.reshape(2, down_weight.shape[0] // 2, down_weight.shape[1])
    return layer(
        queries, keys, values, query_gain[None, :], key_norm_gain[None, :], out_weight,
        residual_in, mlp_gain[None, :], gate_weight, up_weight, down, n_sp, n_tp,
    )


def solution(mesh):
    in_specs = (
        P("sp", "tp"),
        P("sp", "tp"),
        P("sp", None),
        P("sp", None),
        P(),
        P(),
        P("tp", None),
        P(),
        P("sp", "tp"),
        P("sp", "tp"),
        P("tp", "sp"),
    )
    out_specs = P("sp", "tp")
    return jax.shard_map(
        functools.partial(on_device, mesh.shape["sp"], mesh.shape["tp"]),
        mesh=mesh, in_specs=in_specs, out_specs=out_specs, check_vma=False,
    )
```
